32 devices in a mesh: grp: 2 (over x), kv: 4 (over z), tp: 4 (over y, core).
Axes of the slice: x: 2, y: 2, z: 4, core: 2. Of those that a mesh axis runs over, the one named last changes fastest.
Arguments:
- x_rows: bfloat16 [256, 4096], P('grp', 'kv'), parts along dimension 0, may hold values from -32 to 32
- in_gain: bfloat16 [4096], P('kv'), may hold values from 0.099609375 to 1.8984375
- query_weight: bfloat16 [4096, 4096], P('kv', 'tp'), may hold values from -0.09375 to 0.09375
- key_weight: bfloat16 [4096, 4096], P('kv', 'tp'), may hold values from -0.09375 to 0.09375
- value_weight: bfloat16 [4096, 8192], P('kv', 'tp'), may hold values from -0.09375 to 0.09375
- outgate_weight: bfloat16 [4096, 8192], P('kv', 'tp'), may hold values from -0.09375 to 0.09375
- input_gate_weight: bfloat16 [4096, 32], P('kv', 'tp'), may hold values from -0.09375 to 0.09375
- forget_gate_weight: bfloat16 [4096, 32], P('kv', 'tp'), may hold values from -0.09375 to 0.09375
- forget_bias: float32 [32], P('tp'), may hold values from -1 to 3
- state_matrix: float32 [256, 32, 128, 256], P(('grp', 'kv'), 'tp'), parts along dimension 0, may hold values from -3 to 3
- state_norm: float32 [256, 32, 128], P(('grp', 'kv'), 'tp'), parts along dimension 0, may hold values from -6 to 6
- state_max: float32 [256, 32], P(('grp', 'kv'), 'tp'), parts along dimension 0, may hold values from -1 to 1
- head_gain: bfloat16 [8192], P('tp'), may hold values from 0.099609375 to 1.8984375
- out_weight: bfloat16 [8192, 4096], P('tp', 'kv'), may hold values from -0.0625 to 0.0625
- mix_gain: bfloat16 [4096], P('kv'), may hold values from 0.099609375 to 1.8984375
- up_weight: bfloat16 [4096, 16384], P('kv', 'tp'), may hold values from -0.09375 to 0.09375
- down_weight: bfloat16 [16384, 4096], P('tp', 'kv'), may hold values from -0.046875 to 0.046875
Outputs:
- mixed_out: bfloat16 [256, 4096], P('grp', 'kv'), parts along dimension 0
- new_matrix: float32 [256, 32, 128, 256], P(('grp', 'kv'), 'tp'), parts along dimension 0
- new_norm: float32 [256, 32, 128], P(('grp', 'kv'), 'tp'), parts along dimension 0
- new_max: float32 [256, 32], P(('grp', 'kv'), 'tp'), parts along dimension 0
The draws below stay inside these ranges and needn't reach their ends.
There are 2 independent parts, one for each index of `grp`. The reference program is written for one: setup_inputs(seed, part) draws one part's arguments, and reference() takes and returns one part's arrays. A program takes and returns all parts, laid end to end along the dimension named above; an argument that names none is the same for every part. Nothing has to cross between parts.
All inputs are finite; a program needn't handle non-finite values.
Results may differ from the reference program's by a relative error of at most 0.019.
Values may be sent and summed in bfloat16 or wider, within the bound.
A program may use at most 192 MiB of HBM per device.

```python
import jax
import jax.numpy as jnp
from jax import lax

D = 4096
H = 32
DQK = 128
DV = 256
FF = 16384
B = 128


def draw_x_rows(key, part):
    first, second, third = jax.random.split(key, 3)
    position = jnp.arange(D, dtype=jnp.float32) / (D - 1)
    rough = jnp.exp(jax.random.uniform(second, (D,), jnp.float32, -0.35, 0.35))
    row_scale = jnp.exp(jax.random.uniform(third, (B, 1), jnp.float32, jnp.log(0.1), jnp.log(1.0)))
    base = jnp.clip(jax.random.normal(first, (B, D), jnp.float32), -4.0, 4.0)
    rising = jnp.exp(jnp.log(3.0) * position)
    return (base * row_scale * (rising * rough)[None, :]).astype(jnp.bfloat16)


def block_scale(key, extent, cuts, low, high):
    def one(dim, blocks):
        heights = jax.random.uniform(jax.random.fold_in(jax.random.fold_in(key, 6), dim), (blocks,), jnp.float32, low / len(cuts), high / len(cuts))
        return jnp.repeat(jnp.exp(heights), extent[dim] // blocks).reshape((-1,) + (1,) * (len(extent) - dim - 1))

    level = one(*cuts[0])
    for cut in cuts[1:]:
        level = level * one(*cut)
    return level


def centred(key, extent, scale, limit, cuts=(), kind=jnp.bfloat16):
    drawn = scale * jax.random.normal(key, extent, jnp.float32)
    if cuts:
        drawn = drawn * block_scale(key, extent, cuts, -0.22, 0.18)
    return jnp.clip(drawn, -limit, limit).astype(kind)


def setup_inputs(seed: int = 0, part: int = 0) -> dict:
    streams_of = jax.random.split(jax.random.key(seed), 18)
    part_splits = jax.random.split(jax.random.fold_in(streams_of[17], part), 18)
    return {
        "x_rows": draw_x_rows(jax.random.fold_in(jax.random.fold_in(streams_of[17], part), 71), part),
        "in_gain": jnp.clip(1.0 + 0.18 * jax.random.normal(streams_of[1], (D,), jnp.float32), 0.099609375, 1.8984375).astype(jnp.bfloat16),
        "query_weight": centred(streams_of[2], (D, H * DQK), D ** -0.5, 0.09375, ((0, 4), (1, 4))),
        "key_weight": centred(streams_of[3], (D, H * DQK), D ** -0.5, 0.09375, ((0, 4), (1, 4))),
        "value_weight": centred(streams_of[4], (D, H * DV), D ** -0.5, 0.09375, ((0, 4), (1, 4))),
        "outgate_weight": centred(streams_of[5], (D, H * DV), D ** -0.5, 0.09375, ((0, 4), (1, 4))),
        "input_gate_weight": centred(streams_of[6], (D, H), D ** -0.5, 0.09375, ((0, 4), (1, 4))),
        "forget_gate_weight": centred(streams_of[7], (D, H), D ** -0.5, 0.09375, ((0, 4), (1, 4))),
        "forget_bias": jnp.clip(-1.0 + 4.0 * jax.random.uniform(streams_of[8], (H,), jnp.float32) ** block_scale(streams_of[8], (H,), ((0, 4),), -0.2, 0.2), -1.0, 3.0),
        "state_matrix": centred(part_splits[9], (B, H, DQK, DV), 0.5, 3.0, ((0, 4), (1, 4)), jnp.float32),
        "state_norm": centred(part_splits[10], (B, H, DQK), 1.0, 6.0, ((0, 4), (1, 4)), jnp.float32),
        "state_max": jnp.clip(jax.random.uniform(part_splits[11], (B, H), jnp.float32, -1.0, 1.0) * block_scale(part_splits[11], (B, H), ((0, 4), (1, 4)), -0.4, 0.0), -1.0, 1.0),
        "head_gain": jnp.clip(1.0 + 0.18 * jax.random.normal(streams_of[12], (H * DV,), jnp.float32), 0.099609375, 1.8984375).astype(jnp.bfloat16),
        "out_weight": centred(streams_of[13], (H * DV, D), (H * DV) ** -0.5, 0.0625, ((0, 4), (1, 4))),
        "mix_gain": jnp.clip(1.0 + 0.18 * jax.random.normal(streams_of[14], (D,), jnp.float32), 0.099609375, 1.8984375).astype(jnp.bfloat16),
        "up_weight": centred(streams_of[15], (D, FF), D ** -0.5, 0.09375, ((0, 4), (1, 4))),
        "down_weight": centred(streams_of[16], (FF, D), FF ** -0.5, 0.046875, ((0, 4), (1, 4))),
    }


epsilon = 1e-06

def reference(x_rows, in_gain, query_weight, key_weight, value_weight, outgate_weight, input_gate_weight, forget_gate_weight, forget_bias, state_matrix, state_norm, state_max, head_gain, out_weight, mix_gain, up_weight, down_weight):
    xfull = x_rows.astype(jnp.float32)
    squares = lax.optimization_barrier(jnp.sum(xfull * xfull, axis=1))
    scale = lax.rsqrt(squares / D + epsilon)[:, None]
    scaled = (xfull * in_gain.astype(jnp.float32)).astype(jnp.bfloat16)

    def project(weight):
        return jnp.dot(scaled, weight, preferred_element_type=jnp.float32) * scale

    def rounded(weight):
        return lax.optimization_barrier(project(weight).astype(jnp.bfloat16)).astype(jnp.float32)
    query = rounded(query_weight).reshape(B, H, DQK) * DQK ** (-0.5)
    keys = rounded(key_weight).reshape(B, H, DQK)
    values = rounded(value_weight).reshape(B, H, DV)
    outgate = rounded(outgate_weight).reshape(B, H, DV)
    igate = project(input_gate_weight)
    fgate = project(forget_gate_weight)
    log_forget = jax.nn.log_sigmoid(fgate + forget_bias[None, :])
    new_max = jnp.maximum(log_forget + state_max, igate)
    fdecay = jnp.exp(log_forget + state_max - new_max)
    idecay = jnp.exp(igate - new_max)
    new_matrix = fdecay[:, :, None, None] * state_matrix + idecay[:, :, None, None] * (keys[:, :, :, None] * values[:, :, None, :])
    new_norm = fdecay[:, :, None] * state_norm + idecay[:, :, None] * keys
    numer = jnp.einsum('bhd,bhde->bhe', query, new_matrix, precision=lax.Precision.HIGHEST)
    denom = lax.optimization_barrier(jnp.sum(query * new_norm, axis=-1))
    readout = numer / jnp.maximum(jnp.abs(denom), jnp.exp(-new_max))[:, :, None]
    normed = readout * lax.rsqrt(lax.optimization_barrier(jnp.mean(readout * readout, axis=-1, keepdims=True)) + epsilon)
    normed = normed * head_gain.astype(jnp.float32).reshape(H, DV)
    merged = (jax.nn.sigmoid(outgate) * normed).reshape(B, H * DV).astype(jnp.bfloat16)
    branch = jnp.dot(merged, out_weight, preferred_element_type=jnp.float32)
    resid = lax.optimization_barrier((xfull + branch).astype(jnp.bfloat16)).astype(jnp.float32)
    scale_two = lax.rsqrt(lax.optimization_barrier(jnp.sum(resid * resid, axis=1)) / D + epsilon)[:, None]
    scaled_two = (resid * mix_gain.astype(jnp.float32)).astype(jnp.bfloat16)
    act = jnp.dot(scaled_two, up_weight, preferred_element_type=jnp.float32) * scale_two
    hidden = jnp.square(jax.nn.relu(act)).astype(jnp.bfloat16)
    down = jnp.dot(hidden, down_weight, preferred_element_type=jnp.float32)
    mixed_out = (resid + down).astype(jnp.bfloat16)
    return (mixed_out, new_matrix, new_norm, new_max)
```

```python
import functools

import jax
import jax.numpy as jnp
from jax import lax
from jax.experimental import pallas as pl
from jax.experimental.pallas import tpu as pltpu
from jax.sharding import PartitionSpec as P

LANES = 128
EPS = 1e-06
MESH = pl.DeviceIdType.MESH
F32 = jnp.float32
BF16 = jnp.bfloat16
PIECES = 2
SKEW = 2
UP_SKEW = 3


def kernel(
    kvn,
    tpn,
    width,
    gate_heads,
    up_width,
    x_hbm,
    gain_hbm,
    q_hbm,
    k_hbm,
    v_hbm,
    o_hbm,
    ig_hbm,
    fg_hbm,
    bias_hbm,
    state_hbm,
    norm_hbm,
    max_hbm,
    head_gain_hbm,
    out_hbm,
    mix_gain_hbm,
    up_hbm,
    down_hbm,
    mixed_ref,
    state,
    new_norm_ref,
    new_max_ref,
    x_ref,
    gain_ref,
    ig_ref,
    fg_ref,
    bias_ref,
    norm_ref,
    max_ref,
    head_gain_ref,
    mix_gain_ref,
    weights,
    down_w,
    scaled,
    part,
    gate_send,
    gate_recv,
    max_pad,
    part_send,
    pair_recv,
    cross_recv,
    norm_h,
    fd_all,
    id_all,
    em_all,
    scale_b,
    hg_rows,
    numer_s,
    normed_all,
    merged_all,
    half_send,
    half_recv,
    y_send,
    y_recv,
    full,
    sq_send,
    sq_recv,
    scale_two,
    upb,
    up_cross,
    small_sem,
    w_sem,
    w2_sem,
    down_sem,
    state_sem,
    gate_ss,
    gate_rs,
    pair_ss,
    pair_rs,
    cross_ss,
    cross_rs,
    ag_ss,
    relay_ss,
    ag_rs,
    half_ss,
    half_rs,
    y_ss,
    y_rs,
    full_ss,
    full_rs,
    sq_ss,
    sq_rs,
    up_ss,
    up_rs,
    upx_ss,
    upx_rs,
    hid_ss,
    hid_rs,
):
    me = lax.axis_index("kv")
    tme = lax.axis_index("tp")
    total, local = x_ref.shape
    rows, heads, dqk = norm_ref.shape
    dv = v_hbm.shape[1] // heads
    model = local * kvn
    hidden_units = up_hbm.shape[1]
    hp = gate_send.shape[0] // 3
    gate_width = gate_heads * dv
    gate_chunks = heads // gate_heads
    chunks = heads + gate_chunks
    up_chunks = hidden_units // up_width
    npairs = kvn // 2
    pair = me // 2
    partner = me + 1 - 2 * (me % 2)
    lead_bit = 1 - (2 * pair) // npairs
    leader = (me % 2) == lead_bit
    outer = (me % 2) != lead_bit

    def wrap(j):
        return lax.rem(me + j, kvn)

    def remote(src, dst, ssem, rsem, axis, peer):
        return pltpu.make_async_remote_copy(
            src_ref=src,
            dst_ref=dst,
            send_sem=ssem,
            recv_sem=rsem,
            device_id={axis: peer},
            device_id_type=MESH,
        )

    def arrived(dst, rsem, ssem):
        remote(dst, dst, ssem, rsem, "kv", partner).wait_recv()

    def outside():
        for jj in range(1, npairs):
            other = lax.rem(pair + jj, npairs)
            for b in range(2):
                yield jj, b, 2 * other + b

    small = []
    for i, (src, dst) in enumerate(
        (
            (x_hbm, x_ref),
            (gain_hbm, gain_ref),
            (ig_hbm, ig_ref),
            (fg_hbm, fg_ref),
            (bias_hbm, bias_ref),
            (max_hbm, max_ref),
            (norm_hbm, norm_ref),
            (head_gain_hbm, head_gain_ref),
            (mix_gain_hbm, mix_gain_ref),
        )
    ):
        copy = pltpu.make_async_copy(src, dst, small_sem.at[i])
        copy.start()
        small.append(copy)

    def qkv_loads(h):
        found = []
        at = 0
        for i, (ref, extent) in enumerate(((q_hbm, dqk), (k_hbm, dqk), (v_hbm, dv))):
            src = ref.at[:, pl.ds(pl.multiple_of(h * extent, extent), extent)]
            found.append(pltpu.make_async_copy(src, weights.at[h, :, pl.ds(at, extent)], w_sem.at[h, i]))
            at += extent
        return found

    def gate_load(c):
        src = o_hbm.at[:, pl.ds(pl.multiple_of(c * gate_width, gate_width), gate_width)]
        return pltpu.make_async_copy(src, weights.at[heads + c, :, pl.ds(0, gate_width)], w_sem.at[heads + c, 0])

    for h in range(heads):
        for copy in qkv_loads(h):
            copy.start()
    for c in range(gate_chunks):
        gate_load(c).start()

    def state_load(h):
        return pltpu.make_async_copy(state_hbm.at[:, h], state.at[:, h], state_sem.at[h])

    for h in range(heads):
        state_load(h).start()

    tp_steps = []
    s = 1
    while s < tpn:
        tp_steps.append(s)
        s *= 2

    def tp_peer(s):
        return tme + s - 2 * s * ((tme // s) % 2)

    barrier = pltpu.get_barrier_semaphore()
    for j in range(1, kvn):
        pl.semaphore_signal(barrier, inc=1, device_id={"kv": wrap(j)}, device_id_type=MESH)
    for s in tp_steps:
        pl.semaphore_signal(barrier, inc=1, device_id={"tp": tp_peer(s)}, device_id_type=MESH)

    def row_of(ref):
        pieces = [ref[i : i + 1, :].astype(F32) for i in range(ref.shape[0])]
        return jnp.concatenate(pieces, axis=1)

    def lane_row(col):
        return jnp.broadcast_to(col, (total, LANES)).T

    for copy in small[:4]:
        copy.wait()
    xf = x_ref[...].astype(F32)
    squares = jnp.sum(xf * xf, axis=1, keepdims=True)
    scaled[...] = (xf * row_of(gain_ref)).astype(BF16)
    gate_send[...] = jnp.zeros(gate_send.shape, F32)
    contract = (((1,), (1,)), ((), ()))
    for i, ref in enumerate((ig_ref, fg_ref)):
        gate_send[i * hp : i * hp + heads, :] = lax.dot_general(
            ref[...], scaled[...], contract, preferred_element_type=F32
        )
    gate_send[2 * hp : 3 * hp, :] = lane_row(squares)[0:hp, :]
    pl.semaphore_wait(barrier, (kvn - 1) + len(tp_steps))
    gate_copies = [
        remote(gate_send, gate_recv.at[j - 1], gate_ss.at[j - 1], gate_rs.at[j - 1], "kv", wrap(j))
        for j in range(1, kvn)
    ]
    for copy in gate_copies:
        copy.start()

    def block(buf, c, d, wide):
        if wide == width:
            return buf.at[c, d]
        return buf.at[c, d, :, pl.ds(0, wide)]

    def outer_sends(c, wide):
        found = []
        dests = [d for _, _, d in outside()] + [partner]
        for i, d in enumerate(dests):
            found.append(
                remote(
                    block(part_send, c, d, wide),
                    block(pair_recv, c, d, wide),
                    pair_ss.at[c, i],
                    pair_rs.at[c, d],
                    "kv",
                    partner,
                )
            )
        return found

    def inner_send(c, wide):
        return remote(
            block(part_send, c, partner, wide),
            block(pair_recv, c, partner, wide),
            pair_ss.at[c, 0],
            pair_rs.at[c, partner],
            "kv",
            partner,
        )

    def project(c, wide):
        tile = min(256, wide)

        def body(i, carry):
            cols = pl.ds(pl.multiple_of(i * tile, tile), tile)
            res = jnp.dot(scaled[...], weights[c, :, cols], preferred_element_type=F32)
            part_send[c, :, :, cols] = res.reshape(kvn, rows, tile).astype(BF16)
            return carry

        lax.fori_loop(0, wide // tile, body, 0)

        @pl.when(outer)
        def _():
            for copy in outer_sends(c, wide):
                copy.start()

        @pl.when(leader)
        def _():
            inner_send(c, wide).start()

    def qkv_project(h, carry):
        for copy in qkv_loads(h):
            copy.wait()
        project(h, width)
        return carry

    lax.fori_loop(0, heads, qkv_project, 0)

    def gate_project(c, carry):
        gate_load(c).wait()
        project(heads + c, gate_width)
        return carry

    lax.fori_loop(0, gate_chunks, gate_project, 0)

    wide_out = min(width, local)
    second = []
    for a in range(0, out_hbm.shape[0], local):
        for b in range(0, local, wide_out):
            second.append((out_hbm, a, b, wide_out))
    out_blocks = len(second)
    for b in range(0, hidden_units, width):
        second.append((up_hbm, 0, b, width))
    loads2 = []
    for i, (ref, a, b, wide) in enumerate(second):
        copy = pltpu.make_async_copy(
            ref.at[pl.ds(a, local), pl.ds(b, wide)], weights.at[i, :, pl.ds(0, wide)], w2_sem.at[i]
        )
        copy.start()
        loads2.append(copy)
    down_load = pltpu.make_async_copy(down_hbm, down_w, down_sem.at[0])
    down_load.start()

    for copy in small[4:]:
        copy.wait()
    for h in range(heads):
        norm_h[h] = norm_ref[:, h, :]
        n = dv // LANES
        for i in range(n):
            hg_rows[h, :, i * LANES : (i + 1) * LANES] = head_gain_ref[h * n + i : h * n + i + 1, :].astype(F32)
    max_pad[...] = jnp.zeros(max_pad.shape, F32)
    max_pad[0:heads, 0:rows] = max_ref[...]
    spread = jnp.broadcast_to(bias_ref[...], (heads, heads))
    diag = lax.broadcasted_iota(jnp.int32, (heads, heads), 0) == lax.broadcasted_iota(jnp.int32, (heads, heads), 1)
    bias = jnp.sum(jnp.where(diag, spread, 0.0), axis=1, keepdims=True)
    if heads < hp:
        bias = jnp.concatenate([bias, jnp.zeros((hp - heads, 1), F32)], axis=0)
    for copy in gate_copies:
        copy.wait_recv()
    gsum = gate_send[...]
    for j in range(1, kvn):
        gsum = gsum + gate_recv[j - 1]
    gsum = pltpu.roll(gsum, lax.rem(total - me * rows, total), 1)
    scale = lax.rsqrt(gsum[2 * hp : 3 * hp, :] / model + EPS)
    igate = gsum[0:hp, :] * scale
    z = gsum[hp : 2 * hp, :] * scale + bias
    logf = jnp.minimum(z, 0.0) - jnp.log1p(jnp.exp(-jnp.abs(z)))
    held = logf + max_pad[...]
    new_max = jnp.maximum(held, igate)
    new_max_ref[...] = new_max[0:heads, 0:rows]
    fdec = jnp.exp(held - new_max)
    idec = jnp.exp(igate - new_max)
    floor = jnp.exp(-new_max)
    stacked = jnp.concatenate([fdec, idec, floor, scale, jnp.zeros((LANES - 4 * hp, total), F32)], axis=0).T
    for h in range(heads):
        for i, dst in enumerate((fd_all, id_all, em_all)):
            at = i * hp + h
            dst[h] = jnp.broadcast_to(stacked[0:rows, at : at + 1], (rows, LANES))
    scale_b[...] = jnp.broadcast_to(stacked[0:rows, 3 * hp : 3 * hp + 1], (rows, LANES))

    def cross_sends(c, wide):
        found = []
        for jj, b, d in outside():
            slot = npairs - jj - 1
            found.append(
                (
                    d,
                    remote(
                        block(pair_recv, c, d, wide),
                        block(cross_recv, c, slot, wide),
                        cross_ss.at[c, (jj - 1) * 2 + b],
                        cross_rs.at[c, slot],
                        "kv",
                        d,
                    ),
                )
            )
        return found

    def combine(c, wide):
        for d, copy in cross_sends(c, wide):
            arrived(block(pair_recv, c, d, wide), pair_rs.at[c, d], pair_ss.at[c, 0])
            cols = pl.ds(0, wide)
            both = part_send[c, d, :, cols].astype(F32) + pair_recv[c, d, :, cols].astype(F32)
            pair_recv[c, d, :, cols] = both.astype(BF16)
            copy.start()

    def combine_any(c):
        @pl.when(leader)
        def _():
            if gate_width == width:

                @pl.when(c < chunks)
                def _():
                    combine(c, width)

            else:

                @pl.when(c < heads)
                def _():
                    combine(c, width)

                @pl.when(jnp.logical_and(c >= heads, c < chunks))
                def _():
                    combine(c, gate_width)

    def summed(c, wide):
        arrived(block(pair_recv, c, me, wide), pair_rs.at[c, me], pair_ss.at[c, 0])
        for i in range(npairs - 1):
            arrived(block(cross_recv, c, i, wide), cross_rs.at[c, i], pair_ss.at[c, 0])
        found = []
        for g in range(0, wide, LANES):
            cols = pl.ds(g, LANES)
            val = part_send[c, me, :, cols].astype(F32) + pair_recv[c, me, :, cols].astype(F32)
            for i in range(npairs - 1):
                val = val + cross_recv[c, i, :, cols].astype(F32)
            found.append((val * scale_b[...]).astype(BF16).astype(F32))
        return found

    for c in range(SKEW):
        combine_any(c)

    def head_body(h, carry):
        combine_any(h + SKEW)
        cols = summed(h, width)
        nq = dqk // LANES
        q = jnp.concatenate(cols[:nq], axis=1) * (dqk ** (-0.5))
        k = jnp.concatenate(cols[nq : 2 * nq], axis=1)
        v = jnp.concatenate(cols[2 * nq :], axis=1)
        fd = fd_all[h]
        ik = id_all[h] * k
        nn = fd * norm_h[h] + ik
        norm_h[h] = nn
        denom = jnp.sum(q * nn, axis=1, keepdims=True)
        pad = jnp.zeros((LANES - 2 * rows, dqk), F32)
        turned = jnp.concatenate([ik, q, pad], axis=0).T
        wide_fd = jnp.concatenate([fd] * (dv // LANES), axis=1)
        state_load(h).wait()
        for r in range(rows):
            new = wide_fd[r : r + 1, :] * state[r, h] + turned[:, r : r + 1] * v[r : r + 1, :]
            state[r, h] = new
            numer_s[r : r + 1, :] = jnp.sum(turned[:, rows + r : rows + r + 1] * new, axis=0, keepdims=True)
        readout = numer_s[...] / jnp.maximum(jnp.abs(denom), em_all[h][:, 0:1])
        normed = readout * lax.rsqrt(jnp.sum(readout * readout, axis=1, keepdims=True) / dv + EPS)
        normed_all[h] = normed * hg_rows[h]
        return carry

    lax.fori_loop(0, heads, head_body, 0)

    def own_sends(c):
        src = merged_all.at[c, me]
        return [
            remote(src, src, ag_ss.at[c, j - 1], ag_rs.at[c, me], "kv", wrap(j)) for j in range(1, kvn)
        ]

    def outer_own(c):
        src = merged_all.at[c, me]
        return remote(src, src, ag_ss.at[c, 0], ag_rs.at[c, me], "kv", partner)

    def relay_sends(c):
        src = merged_all.at[c, partner]
        return [
            remote(src, src, relay_ss.at[c, (jj - 1) * 2 + b], ag_rs.at[c, partner], "kv", d)
            for jj, b, d in outside()
        ]

    def relay(c):
        @pl.when(leader)
        def _():
            arrived(merged_all.at[c, partner], ag_rs.at[c, partner], ag_ss.at[c, 0])
            for copy in relay_sends(c):
                copy.start()

    def gate_body(c):
        combine_any(heads + c + SKEW)
        cols = summed(heads + c, gate_width)
        n = dv // LANES
        for i in range(gate_heads):
            o = jnp.concatenate(cols[i * n : (i + 1) * n], axis=1)
            val = jax.nn.sigmoid(o) * normed_all[c * gate_heads + i]
            merged_all[c, me, :, i * dv : (i + 1) * dv] = val.astype(BF16)

        @pl.when(leader)
        def _():
            for copy in own_sends(c):
                copy.start()

        @pl.when(outer)
        def _():
            outer_own(c).start()

    def out_project(c):
        @pl.when(outer)
        def _():
            arrived(merged_all.at[c, partner], ag_rs.at[c, partner], ag_ss.at[c, 0])

        for _, _, d in outside():
            arrived(merged_all.at[c, d], ag_rs.at[c, d], ag_ss.at[c, 0])
        tile = min(256, wide_out)
        lhs = merged_all[c].reshape(total, gate_width)
        for i, (ref, a, b, wide) in enumerate(second[:out_blocks]):
            if not a <= c * gate_width < a + local:
                continue
            if c * gate_width == a:
                loads2[i].wait()

            def body(t, carry, i=i, a=a, b=b):
                cols = pl.ds(pl.multiple_of(t * tile, tile), tile)
                into = pl.ds(pl.multiple_of(b + t * tile, tile), tile)
                w = weights[i, c * gate_width - a : (c + 1) * gate_width - a, cols]
                res = jnp.dot(lhs, w, preferred_element_type=F32)
                if c == 0:
                    part[:, into] = res
                else:
                    part[:, into] += res
                return carry

            lax.fori_loop(0, wide // tile, body, 0)

    for c in range(gate_chunks):
        gate_body(c)
        if c >= 1:
            relay(c - 1)
        if c >= 2:
            out_project(c - 2)
    relay(gate_chunks - 1)
    for c in range(max(gate_chunks - 2, 0), gate_chunks):
        out_project(c)

    half = total // 2
    piece = local // PIECES
    low = tme % 2
    mate = tme + 1 - 2 * low
    mine = pl.ds(pl.multiple_of(low * half, half), half)
    theirs = pl.ds(pl.multiple_of((1 - low) * half, half), half)

    def tp_sum(n, base):
        sent = []
        stage = []
        for p in range(PIECES):
            cols = slice(p * piece, (p + 1) * piece)
            half_send[n, p] = part[theirs, cols].astype(BF16)
            copy = remote(half_send.at[n, p], half_recv.at[n, p], half_ss.at[n, p], half_rs.at[n, p], "tp", mate)
            copy.start()
            stage.append(copy)
        sent += stage
        for p in range(PIECES):
            cols = slice(p * piece, (p + 1) * piece)
            stage[p].wait_recv()
            val = part[mine, cols] + half_recv[n, p].astype(F32)
            if len(tp_steps) > 1:
                y_send[n, 0, p] = val.astype(BF16)
            else:
                full[n, low, p] = (base(p) + val).astype(BF16)
        for i, s in enumerate(tp_steps[1:]):
            stage = []
            for p in range(PIECES):
                copy = remote(
                    y_send.at[n, i, p], y_recv.at[n, i, p], y_ss.at[n, i, p], y_rs.at[n, i, p], "tp", tp_peer(s)
                )
                copy.start()
                stage.append(copy)
            sent += stage
            for p in range(PIECES):
                stage[p].wait_recv()
                val = y_send[n, i, p].astype(F32) + y_recv[n, i, p].astype(F32)
                if i + 2 < len(tp_steps):
                    y_send[n, i + 1, p] = val.astype(BF16)
                else:
                    full[n, low, p] = (base(p) + val).astype(BF16)
        stage = []
        for p in range(PIECES):
            src = full.at[n, low, p]
            copy = remote(src, src, full_ss.at[n, p], full_rs.at[n, p], "tp", mate)
            copy.start()
            stage.append(copy)
        for copy in stage:
            copy.wait_recv()
        return sent + stage

    sent = tp_sum(0, lambda p: x_ref[mine, p * piece : (p + 1) * piece].astype(F32))
    mix_row = row_of(mix_gain_ref)
    sq = jnp.zeros((total, 1), F32)
    for p in range(PIECES):
        cols = slice(p * piece, (p + 1) * piece)
        rf = jnp.concatenate([full[0, 0, p], full[0, 1, p]], axis=0).astype(F32)
        sq = sq + jnp.sum(rf * rf, axis=1, keepdims=True)
        scaled[:, cols] = (rf * mix_row[:, cols]).astype(BF16)
    sq_send[...] = lane_row(sq)[0:8, :]
    sq_copies = [
        remote(sq_send, sq_recv.at[j - 1], sq_ss.at[j - 1], sq_rs.at[j - 1], "kv", wrap(j)) for j in range(1, kvn)
    ]
    for copy in sq_copies:
        copy.start()

    for copy in loads2[out_blocks:]:
        copy.wait()
    per_slot = width // up_width

    def outer_up(c):
        return remote(upb.at[0, c], upb.at[1, c], up_ss.at[c], up_rs.at[c], "kv", partner)

    def up_body(c, carry):
        slot = out_blocks + c // per_slot
        cols = pl.ds(pl.multiple_of((c % per_slot) * up_width, up_width), up_width)
        upb[0, c] = jnp.dot(scaled[...], weights[slot, :, cols], preferred_element_type=F32).astype(BF16)

        @pl.when(outer)
        def _():
            outer_up(c).start()

        return carry

    lax.fori_loop(0, up_chunks, up_body, 0)
    for copy in sq_copies:
        copy.wait_recv()
    sq_sum = sq_send[...]
    for j in range(1, kvn):
        sq_sum = sq_sum + sq_recv[j - 1]
    two = lax.rsqrt(sq_sum[0:1, :] / model + EPS)
    scale_two[...] = jnp.broadcast_to(two, (LANES, total)).T

    def up_cross_sends(c):
        found = []
        for jj in range(1, npairs):
            other = lax.rem(pair + jj, npairs)
            head = 2 * other + 1 - (2 * other) // npairs
            slot = npairs - jj - 1
            found.append(
                remote(upb.at[1, c], up_cross.at[c, slot], upx_ss.at[c, jj - 1], upx_rs.at[c, slot], "kv", head)
            )
        return found

    def hidden_send(c):
        return remote(upb.at[0, c], upb.at[1, c], hid_ss.at[c], hid_rs.at[c], "kv", partner)

    def up_combine(c):
        arrived(upb.at[1, c], up_rs.at[c], up_ss.at[c])
        both = upb[0, c].astype(F32) + upb[1, c].astype(F32)
        upb[1, c] = both.astype(BF16)
        for copy in up_cross_sends(c):
            copy.start()

    def up_finish(c):
        for i in range(npairs - 1):
            arrived(up_cross.at[c, i], upx_rs.at[c, i], up_ss.at[c])
        for g in range(0, up_width, LANES):
            cols = pl.ds(g, LANES)
            val = upb[1, c, :, cols].astype(F32)
            for i in range(npairs - 1):
                val = val + up_cross[c, i, :, cols].astype(F32)
            act = jnp.maximum(val * scale_two[...], 0.0)
            upb[0, c, :, cols] = (act * act).astype(BF16)
        hidden_send(c).start()

    down_load.wait()
    down_tile = min(256, local)
    part[...] = jnp.zeros(part.shape, F32)

    def down_project(c, which):
        rws = pl.ds(pl.multiple_of(c * up_width, up_width), up_width)

        def body(t, carry):
            cols = pl.ds(pl.multiple_of(t * down_tile, down_tile), down_tile)
            part[:, cols] += jnp.dot(upb[which, c], down_w[rws, cols], preferred_element_type=F32)
            return carry

        lax.fori_loop(0, local // down_tile, body, 0)

    @pl.when(leader)
    def _():
        def tick(c, carry):
            @pl.when(c < up_chunks)
            def _():
                up_combine(c)

            @pl.when(c >= UP_SKEW)
            def _():
                up_finish(c - UP_SKEW)
                down_project(c - UP_SKEW, 0)

            return carry

        lax.fori_loop(0, up_chunks + UP_SKEW, tick, 0)

    @pl.when(outer)
    def _():
        def tick(c, carry):
            arrived(upb.at[1, c], hid_rs.at[c], up_ss.at[c])
            down_project(c, 1)
            return carry

        lax.fori_loop(0, up_chunks, tick, 0)

    def resid(p):
        return full[0, low, p].astype(F32)

    sent += tp_sum(1, resid)
    for p in range(PIECES):
        cols = slice(p * piece, (p + 1) * piece)
        for b in range(2):
            mixed_ref[b * half : (b + 1) * half, cols] = full[1, b, p]
    for h in range(heads):
        new_norm_ref[:, h, :] = norm_h[h]

    for copy in sent + gate_copies + sq_copies:
        copy.wait_send()

    def drain(c, wide):
        @pl.when(outer)
        def _():
            for copy in outer_sends(c, wide):
                copy.wait_send()

        @pl.when(leader)
        def _():
            inner_send(c, wide).wait_send()
            for _, copy in cross_sends(c, wide):
                copy.wait_send()

    def drain_qkv(c, carry):
        drain(c, width)
        return carry

    def drain_gate(c, carry):
        drain(heads + c, gate_width)

        @pl.when(outer)
        def _():
            outer_own(c).wait_send()

        @pl.when(leader)
        def _():
            for copy in own_sends(c) + relay_sends(c):
                copy.wait_send()

        return carry

    def drain_up(c, carry):
        @pl.when(outer)
        def _():
            outer_up(c).wait_send()

        @pl.when(leader)
        def _():
            for copy in up_cross_sends(c) + [hidden_send(c)]:
                copy.wait_send()

        return carry

    lax.fori_loop(0, heads, drain_qkv, 0)
    lax.fori_loop(0, gate_chunks, drain_gate, 0)
    lax.fori_loop(0, up_chunks, drain_up, 0)


def flush(*refs):
    sem = refs[-1]
    n = (len(refs) - 1) // 2
    copies = []
    for i in range(1, n):
        copies.append((refs[i], refs[n + i]))
    for r in range(refs[0].shape[0]):
        copies.append((refs[0].at[r], refs[n].at[r]))
    started = []
    for i, (src, dst) in enumerate(copies):
        copy = pltpu.make_async_copy(src, dst, sem.at[i])
        copy.start()
        started.append(copy)
    for copy in started:
        copy.wait()


def per_device(
    kvn,
    tpn,
    x_rows,
    in_gain,
    query_weight,
    key_weight,
    value_weight,
    outgate_weight,
    input_gate_weight,
    forget_gate_weight,
    forget_bias,
    state_matrix,
    state_norm,
    state_max,
    head_gain,
    out_weight,
    mix_gain,
    up_weight,
    down_weight,
):
    total, local = x_rows.shape
    rows, heads, dqk, dv = state_matrix.shape
    hidden_units = up_weight.shape[1]
    width = 2 * dqk + dv
    gate_heads = min(2, heads)
    gate_width = gate_heads * dv
    gate_chunks = heads // gate_heads
    chunks = heads + gate_chunks
    up_width = min(256, width)
    up_chunks = hidden_units // up_width
    wide_out = min(width, local)
    slots2 = (heads * dv // local) * (local // wide_out) + hidden_units // width
    slots = max(chunks, slots2)
    hp = -(-heads // 8) * 8
    npairs = kvn // 2
    np1 = max(npairs - 1, 1)
    steps = max((tpn - 1).bit_length() - 1, 1)
    half, piece = total // 2, local // PIECES
    vmem = pl.BlockSpec(memory_space=pltpu.VMEM)
    hbm = pl.BlockSpec(memory_space=pl.ANY)
    V = pltpu.VMEM
    dma = pltpu.SemaphoreType.DMA
    k1 = kvn - 1
    gains = (local // LANES, LANES)
    hg_shape = (heads * dv // LANES, LANES)
    scratch = [
        V((total, local), BF16),
        V(gains, BF16),
        V((heads, local), BF16),
        V((heads, local), BF16),
        V((1, heads), F32),
        V((rows, heads, dqk), F32),
        V((heads, rows), F32),
        V(hg_shape, BF16),
        V(gains, BF16),
        V((slots, local, width), BF16),
        V((hidden_units, local), BF16),
        V((total, local), BF16),
        V((total, local), F32),
        V((3 * hp, total), F32),
        V((k1, 3 * hp, total), F32),
        V((hp, total), F32),
        V((chunks, kvn, rows, width), BF16),
        V((chunks, kvn, rows, width), BF16),
        V((chunks, np1, rows, width), BF16),
        V((heads, rows, dqk), F32),
        V((heads, rows, LANES), F32),
        V((heads, rows, LANES), F32),
        V((heads, rows, LANES), F32),
        V((rows, LANES), F32),
        V((heads, 1, dv), F32),
        V((rows, dv), F32),
        V((heads, rows, dv), F32),
        V((gate_chunks, kvn, rows, gate_width), BF16),
        V((2, PIECES, half, piece), BF16),
        V((2, PIECES, half, piece), BF16),
        V((2, steps, PIECES, half, piece), BF16),
        V((2, steps, PIECES, half, piece), BF16),
        V((2, 2, PIECES, half, piece), BF16),
        V((8, total), F32),
        V((k1, 8, total), F32),
        V((total, LANES), F32),
        V((2, up_chunks, total, up_width), BF16),
        V((up_chunks, np1, total, up_width), BF16),
        dma((9,)),
        dma((chunks, 3)),
        dma((slots2,)),
        dma((1,)),
        dma((heads,)),
        dma((k1,)),
        dma((k1,)),
        dma((chunks, k1)),
        dma((chunks, kvn)),
        dma((chunks, 2 * np1)),
        dma((chunks, np1)),
        dma((gate_chunks, k1)),
        dma((gate_chunks, 2 * np1)),
        dma((gate_chunks, kvn)),
        dma((2, PIECES)),
        dma((2, PIECES)),
        dma((2, steps, PIECES)),
        dma((2, steps, PIECES)),
        dma((2, PIECES)),
        dma((2, PIECES)),
        dma((k1,)),
        dma((k1,)),
        dma((up_chunks,)),
        dma((up_chunks,)),
        dma((up_chunks, np1)),
        dma((up_chunks, np1)),
        dma((up_chunks,)),
        dma((up_chunks,)),
    ]
    state_bytes = state_matrix.size * 4
    outs = pl.pallas_call(
        functools.partial(kernel, kvn, tpn, width, gate_heads, up_width),
        out_shape=(
            pltpu.VMEM((total, local), BF16),
            pltpu.VMEM(state_matrix.shape, F32),
            pltpu.VMEM(state_norm.shape, F32),
            pltpu.VMEM((heads, rows), F32),
        ),
        in_specs=[hbm] * 17,
        out_specs=(vmem,) * 4,
        scratch_shapes=scratch,
        compiler_params=pltpu.CompilerParams(
            collective_id=0,
            has_side_effects=True,
            vmem_limit_bytes=67043328 - state_bytes - (1 << 19),
        ),
    )(
        x_rows,
        in_gain.reshape(gains),
        query_weight,
        key_weight,
        value_weight,
        outgate_weight,
        input_gate_weight.T,
        forget_gate_weight.T,
        forget_bias.reshape(1, heads),
        state_matrix,
        state_norm,
        state_max.T,
        head_gain.reshape(hg_shape),
        out_weight,
        mix_gain.reshape(gains),
        up_weight,
        down_weight,
    )
    mixed, new_matrix, new_norm, new_max = outs
    new_matrix, mixed, new_norm, new_max = pl.pallas_call(
        flush,
        out_shape=(
            jax.ShapeDtypeStruct(state_matrix.shape, F32),
            jax.ShapeDtypeStruct((total, local), BF16),
            jax.ShapeDtypeStruct(state_norm.shape, F32),
            jax.ShapeDtypeStruct((heads, rows), F32),
        ),
        in_specs=[hbm] * 4,
        out_specs=(hbm,) * 4,
        scratch_shapes=[dma((rows + 3,))],
        compiler_params=pltpu.CompilerParams(vmem_limit_bytes=1 << 20),
    )(new_matrix, mixed, new_norm, new_max)
    return (mixed, new_matrix, new_norm, new_max.T)


def solution(mesh):
    placed = (
        P("grp", "kv"),
        P("kv"),
        P("kv", "tp"),
        P("kv", "tp"),
        P("kv", "tp"),
        P("kv", "tp"),
        P("kv", "tp"),
        P("kv", "tp"),
        P("tp"),
        P(("grp", "kv"), "tp", None, None),
        P(("grp", "kv"), "tp", None),
        P(("grp", "kv"), "tp"),
        P("tp"),
        P("tp", "kv"),
        P("kv"),
        P("kv", "tp"),
        P("tp", "kv"),
    )
    return jax.shard_map(
        functools.partial(per_device, mesh.shape["kv"], mesh.shape["tp"]),
        mesh=mesh,
        in_specs=placed,
        out_specs=(
            P("grp", "kv"),
            P(("grp", "kv"), "tp", None, None),
            P(("grp", "kv"), "tp", None),
            P(("grp", "kv"), "tp"),
        ),
        check_vma=False,
    )
```

```python
import functools

import jax
import jax.numpy as jnp
from jax import lax
from jax.experimental import pallas as pl
from jax.experimental.pallas import tpu as pltpu
from jax.sharding import PartitionSpec as P

LANES = 128
EPS = 1e-06
MESH = pl.DeviceIdType.MESH
F32 = jnp.float32
BF16 = jnp.bfloat16
PIECES = 2
SKEW = 2
UP_SKEW = 2
AHEAD = 5


def kernel(
    kvn,
    tpn,
    width,
    gate_heads,
    up_width,
    x_hbm,
    gain_hbm,
    q_hbm,
    k_hbm,
    v_hbm,
    o_hbm,
    ig_hbm,
    fg_hbm,
    bias_hbm,
    state_hbm,
    norm_hbm,
    max_hbm,
    head_gain_hbm,
    out_hbm,
    mix_gain_hbm,
    up_hbm,
    down_hbm,
    mixed_ref,
    state,
    new_norm_ref,
    new_max_ref,
    x_ref,
    gain_ref,
    ig_ref,
    fg_ref,
    bias_ref,
    norm_ref,
    max_ref,
    head_gain_ref,
    mix_gain_ref,
    weights,
    down_w,
    scaled,
    part,
    gate_send,
    gate_recv,
    max_pad,
    part_send,
    pair_recv,
    cross_recv,
    norm_h,
    fd_all,
    id_all,
    em_all,
    scale_b,
    hg_rows,
    numer_s,
    opened,
    merged_all,
    half_send,
    half_recv,
    y_send,
    y_recv,
    full,
    sq_send,
    sq_recv,
    scale_two,
    upb,
    up_cross,
    small_sem,
    w_sem,
    w2_sem,
    down_sem,
    state_sem,
    gate_ss,
    gate_rs,
    pair_ss,
    pair_rs,
    cross_ss,
    cross_rs,
    ag_ss,
    relay_ss,
    ag_rs,
    half_ss,
    half_rs,
    y_ss,
    y_rs,
    full_ss,
    full_rs,
    sq_ss,
    sq_rs,
    up_ss,
    up_rs,
    upx_ss,
    upx_rs,
    hid_ss,
    hid_rs,
):
    me = lax.axis_index("kv")
    tme = lax.axis_index("tp")
    total, local = x_ref.shape
    rows, heads, dqk = norm_ref.shape
    dv = v_hbm.shape[1] // heads
    model = local * kvn
    hidden_units = up_hbm.shape[1]
    hp = gate_send.shape[0] // 3
    gate_width = gate_heads * dv
    gate_chunks = heads // gate_heads
    chunks = heads + gate_chunks
    up_chunks = hidden_units // up_width
    npairs = kvn // 2
    pair = me // 2
    partner = me + 1 - 2 * (me % 2)
    lead_bit = 1 - (2 * pair) // npairs
    leader = (me % 2) == lead_bit
    outer = (me % 2) != lead_bit

    def wrap(j):
        return lax.rem(me + j, kvn)

    def remote(src, dst, ssem, rsem, axis, peer):
        return pltpu.make_async_remote_copy(
            src_ref=src,
            dst_ref=dst,
            send_sem=ssem,
            recv_sem=rsem,
            device_id={axis: peer},
            device_id_type=MESH,
        )

    def arrived(dst, rsem, ssem):
        remote(dst, dst, ssem, rsem, "kv", partner).wait_recv()

    def outside():
        for jj in range(1, npairs):
            other = lax.rem(pair + jj, npairs)
            for b in range(2):
                yield jj, b, 2 * other + b

    small = []
    for i, (src, dst) in enumerate(
        (
            (x_hbm, x_ref),
            (gain_hbm, gain_ref),
            (ig_hbm, ig_ref),
            (fg_hbm, fg_ref),
            (bias_hbm, bias_ref),
            (max_hbm, max_ref),
            (norm_hbm, norm_ref),
            (head_gain_hbm, head_gain_ref),
            (mix_gain_hbm, mix_gain_ref),
        )
    ):
        small.append(pltpu.make_async_copy(src, dst, small_sem.at[i]))
    for copy in small[:4]:
        copy.start()

    def qkv_loads(h):
        found = []
        at = 0
        for i, (ref, extent) in enumerate(((q_hbm, dqk), (k_hbm, dqk), (v_hbm, dv))):
            src = ref.at[:, pl.ds(pl.multiple_of(h * extent, extent), extent)]
            found.append(pltpu.make_async_copy(src, weights.at[gate_chunks + h, :, pl.ds(at, extent)], w_sem.at[gate_chunks + h, i]))
            at += extent
        return found

    def gate_load(c):
        src = o_hbm.at[:, pl.ds(pl.multiple_of(c * gate_width, gate_width), gate_width)]
        return pltpu.make_async_copy(src, weights.at[c, :, pl.ds(0, gate_width)], w_sem.at[c, 0])

    for c in range(min(1, gate_chunks)):
        gate_load(c).start()

    def state_load(h):
        return pltpu.make_async_copy(state_hbm.at[:, h], state.at[:, h], state_sem.at[h])

    tp_steps = []
    s = 1
    while s < tpn:
        tp_steps.append(s)
        s *= 2

    def tp_peer(s):
        return tme + s - 2 * s * ((tme // s) % 2)

    barrier = pltpu.get_barrier_semaphore()
    for j in range(1, kvn):
        pl.semaphore_signal(barrier, inc=1, device_id={"kv": wrap(j)}, device_id_type=MESH)
    for s in tp_steps:
        pl.semaphore_signal(barrier, inc=1, device_id={"tp": tp_peer(s)}, device_id_type=MESH)

    def row_of(ref):
        pieces = [ref[i : i + 1, :].astype(F32) for i in range(ref.shape[0])]
        return jnp.concatenate(pieces, axis=1)

    def lane_row(col):
        return jnp.broadcast_to(col, (total, LANES)).T

    for copy in small[:4]:
        copy.wait()
    for c in range(1, gate_chunks):
        gate_load(c).start()
    for h in range(heads):
        for copy in qkv_loads(h):
            copy.start()
    for copy in small[4:]:
        copy.start()
    xf = x_ref[...].astype(F32)
    squares = jnp.sum(xf * xf, axis=1, keepdims=True)
    scaled[...] = (xf * row_of(gain_ref)).astype(BF16)
    gate_send[...] = jnp.zeros(gate_send.shape, F32)
    contract = (((1,), (1,)), ((), ()))
    for i, ref in enumerate((ig_ref, fg_ref)):
        gate_send[i * hp : i * hp + heads, :] = lax.dot_general(
            ref[...], scaled[...], contract, preferred_element_type=F32
        )
    gate_send[2 * hp : 3 * hp, :] = lane_row(squares)[0:hp, :]
    pl.semaphore_wait(barrier, (kvn - 1) + len(tp_steps))
    gate_copies = [
        remote(gate_send, gate_recv.at[j - 1], gate_ss.at[j - 1], gate_rs.at[j - 1], "kv", wrap(j))
        for j in range(1, kvn)
    ]
    for copy in gate_copies:
        copy.start()

    def block(buf, c, d, wide):
        if wide == width:
            return buf.at[c, d]
        return buf.at[c, d, :, pl.ds(0, wide)]

    def outer_sends(c, wide):
        found = []
        dests = [d for _, _, d in outside()] + [partner]
        for i, d in enumerate(dests):
            found.append(
                remote(
                    block(part_send, c, d, wide),
                    block(pair_recv, c, d, wide),
                    pair_ss.at[c, i],
                    pair_rs.at[c, d],
                    "kv",
                    partner,
                )
            )
        return found

    def inner_send(c, wide):
        return remote(
            block(part_send, c, partner, wide),
            block(pair_recv, c, partner, wide),
            pair_ss.at[c, 0],
            pair_rs.at[c, partner],
            "kv",
            partner,
        )

    def project(c, wide):
        tile = min(512, wide)

        def body(i, carry):
            cols = pl.ds(pl.multiple_of(i * tile, tile), tile)
            res = jnp.dot(scaled[...], weights[c, :, cols], preferred_element_type=F32)
            part_send[c, :, :, cols] = res.reshape(kvn, rows, tile).astype(BF16)
            return carry

        lax.fori_loop(0, wide // tile, body, 0)

        @pl.when(jnp.logical_and(outer, c < AHEAD))
        def _():
            for copy in outer_sends(c, wide):
                copy.start()

        @pl.when(leader)
        def _():
            inner_send(c, wide).start()

    def gate_project(c, carry):
        gate_load(c).wait()
        project(c, gate_width)
        return carry

    lax.fori_loop(0, gate_chunks, gate_project, 0)

    def qkv_project(h, carry):
        for copy in qkv_loads(h):
            copy.wait()
        state_load(h).start()
        project(gate_chunks + h, width)
        return carry

    lax.fori_loop(0, heads, qkv_project, 0)

    wide_out = min(width, local)
    second = []
    for a in range(0, out_hbm.shape[0], local):
        for b in range(0, local, wide_out):
            second.append((out_hbm, a, b, wide_out))
    out_blocks = len(second)
    for b in range(0, hidden_units, width):
        second.append((up_hbm, 0, b, width))
    loads2 = []
    for i, (ref, a, b, wide) in enumerate(second):
        copy = pltpu.make_async_copy(
            ref.at[pl.ds(a, local), pl.ds(b, wide)], weights.at[i, :, pl.ds(0, wide)], w2_sem.at[i]
        )
        copy.start()
        loads2.append(copy)
    down_load = pltpu.make_async_copy(down_hbm, down_w, down_sem.at[0])
    down_load.start()

    for copy in small[4:]:
        copy.wait()
    for h in range(heads):
        norm_h[h] = norm_ref[:, h, :]
        n = dv // LANES
        for i in range(n):
            hg_rows[h, :, i * LANES : (i + 1) * LANES] = head_gain_ref[h * n + i : h * n + i + 1, :].astype(F32)
    max_pad[...] = jnp.zeros(max_pad.shape, F32)
    max_pad[0:heads, 0:rows] = max_ref[...]
    spread = jnp.broadcast_to(bias_ref[...], (heads, heads))
    diag = lax.broadcasted_iota(jnp.int32, (heads, heads), 0) == lax.broadcasted_iota(jnp.int32, (heads, heads), 1)
    bias = jnp.sum(jnp.where(diag, spread, 0.0), axis=1, keepdims=True)
    if heads < hp:
        bias = jnp.concatenate([bias, jnp.zeros((hp - heads, 1), F32)], axis=0)
    for copy in gate_copies:
        copy.wait_recv()
    gsum = gate_send[...]
    for j in range(1, kvn):
        gsum = gsum + gate_recv[j - 1]
    gsum = pltpu.roll(gsum, lax.rem(total - me * rows, total), 1)
    scale = lax.rsqrt(gsum[2 * hp : 3 * hp, :] / model + EPS)
    igate = gsum[0:hp, :] * scale
    z = gsum[hp : 2 * hp, :] * scale + bias
    logf = jnp.minimum(z, 0.0) - jnp.log1p(jnp.exp(-jnp.abs(z)))
    held = logf + max_pad[...]
    new_max = jnp.maximum(held, igate)
    new_max_ref[...] = new_max[0:heads, 0:rows]
    fdec = jnp.exp(held - new_max)
    idec = jnp.exp(igate - new_max)
    floor = jnp.exp(-new_max)
    stacked = jnp.concatenate([fdec, idec, floor, scale, jnp.zeros((LANES - 4 * hp, total), F32)], axis=0).T
    for h in range(heads):
        for i, dst in enumerate((fd_all, id_all, em_all)):
            at = i * hp + h
            dst[h] = jnp.broadcast_to(stacked[0:rows, at : at + 1], (rows, LANES))
    scale_b[...] = jnp.broadcast_to(stacked[0:rows, 3 * hp : 3 * hp + 1], (rows, LANES))

    def cross_sends(c, wide):
        found = []
        for jj, b, d in outside():
            slot = npairs - jj - 1
            found.append(
                (
                    d,
                    remote(
                        block(pair_recv, c, d, wide),
                        block(cross_recv, c, slot, wide),
                        cross_ss.at[c, (jj - 1) * 2 + b],
                        cross_rs.at[c, slot],
                        "kv",
                        d,
                    ),
                )
            )
        return found

    def combine(c, wide):
        for d, copy in cross_sends(c, wide):
            arrived(block(pair_recv, c, d, wide), pair_rs.at[c, d], pair_ss.at[c, 0])
            cols = pl.ds(0, wide)
            both = part_send[c, d, :, cols].astype(F32) + pair_recv[c, d, :, cols].astype(F32)
            pair_recv[c, d, :, cols] = both.astype(BF16)
            copy.start()

    def combine_any(c):
        @pl.when(leader)
        def _():
            if gate_width == width:

                @pl.when(c < chunks)
                def _():
                    combine(c, width)

            else:

                @pl.when(c < gate_chunks)
                def _():
                    combine(c, gate_width)

                @pl.when(jnp.logical_and(c >= gate_chunks, c < chunks))
                def _():
                    combine(c, width)

    def send_ahead(c):
        @pl.when(outer)
        def _():
            if gate_width == width:

                @pl.when(c < chunks)
                def _():
                    for copy in outer_sends(c, width):
                        copy.start()

            else:

                @pl.when(c < gate_chunks)
                def _():
                    for copy in outer_sends(c, gate_width):
                        copy.start()

                @pl.when(jnp.logical_and(c >= gate_chunks, c < chunks))
                def _():
                    for copy in outer_sends(c, width):
                        copy.start()

    def summed(c, wide):
        arrived(block(pair_recv, c, me, wide), pair_rs.at[c, me], pair_ss.at[c, 0])
        for i in range(npairs - 1):
            arrived(block(cross_recv, c, i, wide), cross_rs.at[c, i], pair_ss.at[c, 0])
        found = []
        for g in range(0, wide, LANES):
            cols = pl.ds(g, LANES)
            val = part_send[c, me, :, cols].astype(F32) + pair_recv[c, me, :, cols].astype(F32)
            for i in range(npairs - 1):
                val = val + cross_recv[c, i, :, cols].astype(F32)
            found.append((val * scale_b[...]).astype(BF16).astype(F32))
        return found

    last = heads - 1

    def own_sends(h):
        src = merged_all.at[h, me]
        return [
            remote(src, src, ag_ss.at[h, j - 1], ag_rs.at[h, me], "kv", wrap(j)) for j in range(1, kvn)
        ]

    def outer_own(h):
        src = merged_all.at[h, me]
        return remote(src, src, ag_ss.at[h, 0], ag_rs.at[h, me], "kv", partner)

    def relay_sends(h):
        src = merged_all.at[h, partner]
        return [
            remote(src, src, relay_ss.at[h, (jj - 1) * 2 + b], ag_rs.at[h, partner], "kv", d)
            for jj, b, d in outside()
        ]

    def relay(h):
        @pl.when(leader)
        def _():
            arrived(merged_all.at[h, partner], ag_rs.at[h, partner], ag_ss.at[h, 0])
            for copy in relay_sends(h):
                copy.start()

    def spread_merged(h):
        direct = jnp.logical_or(leader, h == last)

        @pl.when(direct)
        def _():
            for copy in own_sends(h):
                copy.start()

        @pl.when(jnp.logical_not(direct))
        def _():
            outer_own(h).start()

    out_tile = min(256, wide_out)
    out_cols = local // wide_out

    def out_project(batch, first):
        for h in batch:
            for _, _, d in outside():
                arrived(merged_all.at[h, d], ag_rs.at[h, d], ag_ss.at[h, 0])

            @pl.when(jnp.logical_or(outer, h == last))
            def _(h=h):
                arrived(merged_all.at[h, partner], ag_rs.at[h, partner], ag_ss.at[h, 0])

        for b in range(out_cols):

            def body(t, carry, b=b):
                cols = pl.ds(pl.multiple_of(t * out_tile, out_tile), out_tile)
                into = pl.ds(pl.multiple_of(b * wide_out + t * out_tile, out_tile), out_tile)
                acc = jnp.zeros((total, out_tile), F32)
                for h in batch:
                    slot = (h * dv // local) * out_cols + b
                    at = (h * dv) % local
                    lhs = merged_all[h].reshape(total, dv)
                    acc = acc + jnp.dot(lhs, weights[slot, at : at + dv, cols], preferred_element_type=F32)
                if first:
                    part[:, into] = acc
                else:
                    part[:, into] += acc
                return carry

            lax.fori_loop(0, wide_out // out_tile, body, 0)

    for c in range(SKEW):
        combine_any(c)

    def gate_body(c, carry):
        combine_any(c + SKEW)
        cols = summed(c, gate_width)
        n = dv // LANES
        for i in range(gate_heads):
            o = jnp.concatenate(cols[i * n : (i + 1) * n], axis=1)
            opened[c * gate_heads + i] = jax.nn.sigmoid(o)
        send_ahead(c + AHEAD)
        return carry

    lax.fori_loop(0, gate_chunks, gate_body, 0)
    def head_body(h, carry):
        combine_any(gate_chunks + h + SKEW)
        cols = summed(gate_chunks + h, width)
        nq = dqk // LANES
        q = jnp.concatenate(cols[:nq], axis=1) * (dqk ** (-0.5))
        k = jnp.concatenate(cols[nq : 2 * nq], axis=1)
        v = jnp.concatenate(cols[2 * nq :], axis=1)
        fd = fd_all[h]
        ik = id_all[h] * k
        nn = fd * norm_h[h] + ik
        norm_h[h] = nn
        denom = jnp.sum(q * nn, axis=1, keepdims=True)
        pad = jnp.zeros((LANES - 2 * rows, dqk), F32)
        turned = jnp.concatenate([ik, q, pad], axis=0).T
        wide_fd = jnp.concatenate([fd] * (dv // LANES), axis=1)
        state_load(h).wait()
        for r in range(rows):
            new = wide_fd[r : r + 1, :] * state[r, h] + turned[:, r : r + 1] * v[r : r + 1, :]
            state[r, h] = new
            numer_s[r : r + 1, :] = jnp.sum(turned[:, rows + r : rows + r + 1] * new, axis=0, keepdims=True)
        readout = numer_s[...] / jnp.maximum(jnp.abs(denom), em_all[h][:, 0:1])
        normed = readout * lax.rsqrt(jnp.sum(readout * readout, axis=1, keepdims=True) / dv + EPS)
        merged_all[h, me] = (opened[h] * (normed * hg_rows[h])).astype(BF16)
        spread_merged(h)

        send_ahead(gate_chunks + h + AHEAD)
        for early in range(last):
            when = min(early + 3, (early + heads + 1) // 2, last)

            @pl.when(h == when)
            def _(early=early):
                relay(early)

        return carry

    lax.fori_loop(0, heads, head_body, 0)
    for copy in loads2[:out_blocks]:
        copy.wait()
    late = max(heads - 2, 0)
    if late:
        out_project(range(late), True)
    out_project(range(late, heads), late == 0)

    half = total // 2
    piece = local // PIECES
    low = tme % 2
    mate = tme + 1 - 2 * low
    mine = pl.ds(pl.multiple_of(low * half, half), half)
    theirs = pl.ds(pl.multiple_of((1 - low) * half, half), half)

    def tp_sum(n, base):
        sent = []
        stage = []
        for p in range(PIECES):
            cols = slice(p * piece, (p + 1) * piece)
            half_send[n, p] = part[theirs, cols].astype(BF16)
            copy = remote(half_send.at[n, p], half_recv.at[n, p], half_ss.at[n, p], half_rs.at[n, p], "tp", mate)
            copy.start()
            stage.append(copy)
        sent += stage
        for p in range(PIECES):
            cols = slice(p * piece, (p + 1) * piece)
            stage[p].wait_recv()
            val = part[mine, cols] + half_recv[n, p].astype(F32)
            if len(tp_steps) > 1:
                y_send[n, 0, p] = val.astype(BF16)
            else:
                full[n, low, p] = (base(p) + val).astype(BF16)
        for i, s in enumerate(tp_steps[1:]):
            stage = []
            for p in range(PIECES):
                copy = remote(
                    y_send.at[n, i, p], y_recv.at[n, i, p], y_ss.at[n, i, p], y_rs.at[n, i, p], "tp", tp_peer(s)
                )
                copy.start()
                stage.append(copy)
            sent += stage
            for p in range(PIECES):
                stage[p].wait_recv()
                val = y_send[n, i, p].astype(F32) + y_recv[n, i, p].astype(F32)
                if i + 2 < len(tp_steps):
                    y_send[n, i + 1, p] = val.astype(BF16)
                else:
                    full[n, low, p] = (base(p) + val).astype(BF16)
        stage = []
        for p in range(PIECES):
            src = full.at[n, low, p]
            copy = remote(src, src, full_ss.at[n, p], full_rs.at[n, p], "tp", mate)
            copy.start()
            stage.append(copy)
        for copy in stage:
            copy.wait_recv()
        return sent + stage

    sent = tp_sum(0, lambda p: x_ref[mine, p * piece : (p + 1) * piece].astype(F32))
    mix_row = row_of(mix_gain_ref)
    sq = jnp.zeros((total, 1), F32)
    for p in range(PIECES):
        cols = slice(p * piece, (p + 1) * piece)
        rf = jnp.concatenate([full[0, 0, p], full[0, 1, p]], axis=0).astype(F32)
        sq = sq + jnp.sum(rf * rf, axis=1, keepdims=True)
        scaled[:, cols] = (rf * mix_row[:, cols]).astype(BF16)
    sq_send[...] = lane_row(sq)[0:8, :]
    sq_copies = [
        remote(sq_send, sq_recv.at[j - 1], sq_ss.at[j - 1], sq_rs.at[j - 1], "kv", wrap(j)) for j in range(1, kvn)
    ]
    for copy in sq_copies:
        copy.start()

    for copy in loads2[out_blocks:]:
        copy.wait()
    per_slot = width // up_width

    def outer_up(c):
        return remote(upb.at[0, c], upb.at[1, c], up_ss.at[c], up_rs.at[c], "kv", partner)

    def up_body(c, carry):
        slot = out_blocks + c // per_slot
        cols = pl.ds(pl.multiple_of((c % per_slot) * up_width, up_width), up_width)
        upb[0, c] = jnp.dot(scaled[...], weights[slot, :, cols], preferred_element_type=F32).astype(BF16)

        @pl.when(outer)
        def _():
            outer_up(c).start()

        return carry

    lax.fori_loop(0, up_chunks, up_body, 0)
    for copy in sq_copies:
        copy.wait_recv()
    sq_sum = sq_send[...]
    for j in range(1, kvn):
        sq_sum = sq_sum + sq_recv[j - 1]
    two = lax.rsqrt(sq_sum[0:1, :] / model + EPS)
    scale_two[...] = jnp.broadcast_to(two, (LANES, total)).T

    def up_cross_sends(c):
        found = []
        for jj in range(1, npairs):
            other = lax.rem(pair + jj, npairs)
            head = 2 * other + 1 - (2 * other) // npairs
            slot = npairs - jj - 1
            found.append(
                remote(upb.at[1, c], up_cross.at[c, slot], upx_ss.at[c, jj - 1], upx_rs.at[c, slot], "kv", head)
            )
        return found

    def hidden_send(c):
        return remote(upb.at[0, c], upb.at[1, c], hid_ss.at[c], hid_rs.at[c], "kv", partner)

    def up_combine(c):
        arrived(upb.at[1, c], up_rs.at[c], up_ss.at[c])
        both = upb[0, c].astype(F32) + upb[1, c].astype(F32)
        upb[1, c] = both.astype(BF16)
        for copy in up_cross_sends(c):
            copy.start()

    def up_finish(c):
        for i in range(npairs - 1):
            arrived(up_cross.at[c, i], upx_rs.at[c, i], up_ss.at[c])
        for g in range(0, up_width, LANES):
            cols = pl.ds(g, LANES)
            val = upb[1, c, :, cols].astype(F32)
            for i in range(npairs - 1):
                val = val + up_cross[c, i, :, cols].astype(F32)
            act = jnp.maximum(val * scale_two[...], 0.0)
            upb[0, c, :, cols] = (act * act).astype(BF16)
        hidden_send(c).start()

    down_load.wait()
    down_tile = min(256, local)
    part[...] = jnp.zeros(part.shape, F32)

    def down_project(c, which):
        rws = pl.ds(pl.multiple_of(c * up_width, up_width), up_width)

        def body(t, carry):
            cols = pl.ds(pl.multiple_of(t * down_tile, down_tile), down_tile)
            part[:, cols] += jnp.dot(upb[which, c], down_w[rws, cols], preferred_element_type=F32)
            return carry

        lax.fori_loop(0, local // down_tile, body, 0)

    @pl.when(leader)
    def _():
        def tick(c, carry):
            @pl.when(c < up_chunks)
            def _():
                up_combine(c)

            @pl.when(c >= UP_SKEW)
            def _():
                up_finish(c - UP_SKEW)
                down_project(c - UP_SKEW, 0)

            return carry

        lax.fori_loop(0, up_chunks + UP_SKEW, tick, 0)

    @pl.when(outer)
    def _():
        def tick(c, carry):
            arrived(upb.at[1, c], hid_rs.at[c], up_ss.at[c])
            down_project(c, 1)
            return carry

        lax.fori_loop(0, up_chunks, tick, 0)

    def resid(p):
        return full[0, low, p].astype(F32)

    sent += tp_sum(1, resid)
    for p in range(PIECES):
        cols = slice(p * piece, (p + 1) * piece)
        for b in range(2):
            mixed_ref[b * half : (b + 1) * half, cols] = full[1, b, p]
    for h in range(heads):
        new_norm_ref[:, h, :] = norm_h[h]

    for copy in sent + gate_copies + sq_copies:
        copy.wait_send()

    def drain(c, wide):
        @pl.when(outer)
        def _():
            for copy in outer_sends(c, wide):
                copy.wait_send()

        @pl.when(leader)
        def _():
            inner_send(c, wide).wait_send()
            for _, copy in cross_sends(c, wide):
                copy.wait_send()

    def drain_gate(c, carry):
        drain(c, gate_width)
        return carry

    def drain_qkv(h, carry):
        drain(gate_chunks + h, width)
        direct = jnp.logical_or(leader, h == last)

        @pl.when(direct)
        def _():
            for copy in own_sends(h):
                copy.wait_send()

        @pl.when(jnp.logical_not(direct))
        def _():
            outer_own(h).wait_send()

        @pl.when(jnp.logical_and(leader, h < last))
        def _():
            for copy in relay_sends(h):
                copy.wait_send()

        return carry

    def drain_up(c, carry):
        @pl.when(outer)
        def _():
            outer_up(c).wait_send()

        @pl.when(leader)
        def _():
            for copy in up_cross_sends(c) + [hidden_send(c)]:
                copy.wait_send()

        return carry

    lax.fori_loop(0, heads, drain_qkv, 0)
    lax.fori_loop(0, gate_chunks, drain_gate, 0)
    lax.fori_loop(0, up_chunks, drain_up, 0)


def flush(*refs):
    sem = refs[-1]
    n = (len(refs) - 1) // 2
    copies = []
    for i in range(1, n):
        copies.append((refs[i], refs[n + i]))
    for r in range(refs[0].shape[0]):
        copies.append((refs[0].at[r], refs[n].at[r]))
    started = []
    for i, (src, dst) in enumerate(copies):
        copy = pltpu.make_async_copy(src, dst, sem.at[i])
        copy.start()
        started.append(copy)
    for copy in started:
        copy.wait()


def per_device(
    kvn,
    tpn,
    x_rows,
    in_gain,
    query_weight,
    key_weight,
    value_weight,
    outgate_weight,
    input_gate_weight,
    forget_gate_weight,
    forget_bias,
    state_matrix,
    state_norm,
    state_max,
    head_gain,
    out_weight,
    mix_gain,
    up_weight,
    down_weight,
):
    total, local = x_rows.shape
    rows, heads, dqk, dv = state_matrix.shape
    hidden_units = up_weight.shape[1]
    width = 2 * dqk + dv
    gate_heads = min(2, heads)
    gate_width = gate_heads * dv
    gate_chunks = heads // gate_heads
    chunks = heads + gate_chunks
    up_width = min(256, width)
    up_chunks = hidden_units // up_width
    wide_out = min(width, local)
    slots2 = (heads * dv // local) * (local // wide_out) + hidden_units // width
    slots = max(chunks, slots2)
    hp = -(-heads // 8) * 8
    npairs = kvn // 2
    np1 = max(npairs - 1, 1)
    steps = max((tpn - 1).bit_length() - 1, 1)
    half, piece = total // 2, local // PIECES
    vmem = pl.BlockSpec(memory_space=pltpu.VMEM)
    hbm = pl.BlockSpec(memory_space=pl.ANY)
    V = pltpu.VMEM
    dma = pltpu.SemaphoreType.DMA
    k1 = kvn - 1
    gains = (local // LANES, LANES)
    hg_shape = (heads * dv // LANES, LANES)
    scratch = [
        V((total, local), BF16),
        V(gains, BF16),
        V((heads, local), BF16),
        V((heads, local), BF16),
        V((1, heads), F32),
        V((rows, heads, dqk), F32),
        V((heads, rows), F32),
        V(hg_shape, BF16),
        V(gains, BF16),
        V((slots, local, width), BF16),
        V((hidden_units, local), BF16),
        V((total, local), BF16),
        V((total, local), F32),
        V((3 * hp, total), F32),
        V((k1, 3 * hp, total), F32),
        V((hp, total), F32),
        V((chunks, kvn, rows, width), BF16),
        V((chunks, kvn, rows, width), BF16),
        V((chunks, np1, rows, width), BF16),
        V((heads, rows, dqk), F32),
        V((heads, rows, LANES), F32),
        V((heads, rows, LANES), F32),
        V((heads, rows, LANES), F32),
        V((rows, LANES), F32),
        V((heads, 1, dv), F32),
        V((rows, dv), F32),
        V((heads, rows, dv), F32),
        V((heads, kvn, rows, dv), BF16),
        V((2, PIECES, half, piece), BF16),
        V((2, PIECES, half, piece), BF16),
        V((2, steps, PIECES, half, piece), BF16),
        V((2, steps, PIECES, half, piece), BF16),
        V((2, 2, PIECES, half, piece), BF16),
        V((8, total), F32),
        V((k1, 8, total), F32),
        V((total, LANES), F32),
        V((2, up_chunks, total, up_width), BF16),
        V((up_chunks, np1, total, up_width), BF16),
        dma((9,)),
        dma((chunks, 3)),
        dma((slots2,)),
        dma((1,)),
        dma((heads,)),
        dma((k1,)),
        dma((k1,)),
        dma((chunks, k1)),
        dma((chunks, kvn)),
        dma((chunks, 2 * np1)),
        dma((chunks, np1)),
        dma((heads, k1)),
        dma((heads, 2 * np1)),
        dma((heads, kvn)),
        dma((2, PIECES)),
        dma((2, PIECES)),
        dma((2, steps, PIECES)),
        dma((2, steps, PIECES)),
        dma((2, PIECES)),
        dma((2, PIECES)),
        dma((k1,)),
        dma((k1,)),
        dma((up_chunks,)),
        dma((up_chunks,)),
        dma((up_chunks, np1)),
        dma((up_chunks, np1)),
        dma((up_chunks,)),
        dma((up_chunks,)),
    ]
    state_bytes = state_matrix.size * 4
    outs = pl.pallas_call(
        functools.partial(kernel, kvn, tpn, width, gate_heads, up_width),
        out_shape=(
            pltpu.VMEM((total, local), BF16),
            pltpu.VMEM(state_matrix.shape, F32),
            pltpu.VMEM(state_norm.shape, F32),
            pltpu.VMEM((heads, rows), F32),
        ),
        in_specs=[hbm] * 17,
        out_specs=(vmem,) * 4,
        scratch_shapes=scratch,
        compiler_params=pltpu.CompilerParams(
            collective_id=0,
            has_side_effects=True,
            vmem_limit_bytes=67043328 - state_bytes - (1 << 19),
        ),
    )(
        x_rows,
        in_gain.reshape(gains),
        query_weight,
        key_weight,
        value_weight,
        outgate_weight,
        input_gate_weight.T,
        forget_gate_weight.T,
        forget_bias.reshape(1, heads),
        state_matrix,
        state_norm,
        state_max.T,
        head_gain.reshape(hg_shape),
        out_weight,
        mix_gain.reshape(gains),
        up_weight,
        down_weight,
    )
    mixed, new_matrix, new_norm, new_max = outs
    new_matrix, mixed = pl.pallas_call(
        flush,
        out_shape=(jax.ShapeDtypeStruct(state_matrix.shape, F32), jax.ShapeDtypeStruct((total, local), BF16)),
        in_specs=[hbm] * 2,
        out_specs=(hbm,) * 2,
        scratch_shapes=[dma((rows + 3,))],
        compiler_params=pltpu.CompilerParams(vmem_limit_bytes=1 << 20),
    )(new_matrix, mixed)
    return (mixed, new_matrix, new_norm, new_max.T)


def solution(mesh):
    placed = (
        P("grp", "kv"),
        P("kv"),
        P("kv", "tp"),
        P("kv", "tp"),
        P("kv", "tp"),
        P("kv", "tp"),
        P("kv", "tp"),
        P("kv", "tp"),
        P("tp"),
        P(("grp", "kv"), "tp", None, None),
        P(("grp", "kv"), "tp", None),
        P(("grp", "kv"), "tp"),
        P("tp"),
        P("tp", "kv"),
        P("kv"),
        P("kv", "tp"),
        P("tp", "kv"),
    )
    return jax.shard_map(
        functools.partial(per_device, mesh.shape["kv"], mesh.shape["tp"]),
        mesh=mesh,
        in_specs=placed,
        out_specs=(
            P("grp", "kv"),
            P(("grp", "kv"), "tp", None, None),
            P(("grp", "kv"), "tp", None),
            P(("grp", "kv"), "tp"),
        ),
        check_vma=False,
    )
```

```python
import functools

import jax
import jax.numpy as jnp
from jax import lax
from jax.experimental import pallas as pl
from jax.experimental.pallas import tpu as pltpu
from jax.sharding import PartitionSpec as P

LANES = 128
EPS = 1e-06
MESH = pl.DeviceIdType.MESH
F32 = jnp.float32
BF16 = jnp.bfloat16
PIECES = 2
SKEW = 2
UP_SKEW = 2
AHEAD = 5


def kernel(
    kvn,
    tpn,
    width,
    gate_heads,
    up_width,
    x_hbm,
    gain_hbm,
    q_hbm,
    k_hbm,
    v_hbm,
    o_hbm,
    ig_hbm,
    fg_hbm,
    bias_hbm,
    state_hbm,
    norm_hbm,
    max_hbm,
    head_gain_hbm,
    out_hbm,
    mix_gain_hbm,
    up_hbm,
    down_hbm,
    mixed_ref,
    state,
    new_norm_ref,
    new_max_ref,
    x_ref,
    gain_ref,
    ig_ref,
    fg_ref,
    bias_ref,
    norm_ref,
    max_ref,
    head_gain_ref,
    mix_gain_ref,
    weights,
    down_w,
    scaled,
    part,
    gate_send,
    gate_recv,
    max_pad,
    part_send,
    pair_recv,
    cross_recv,
    norm_h,
    fd_all,
    id_all,
    em_all,
    scale_b,
    hg_rows,
    numer_s,
    opened,
    merged_all,
    half_send,
    half_recv,
    y_send,
    y_recv,
    full,
    sq_send,
    sq_recv,
    scale_two,
    upb,
    up_cross,
    small_sem,
    w_sem,
    w2_sem,
    down_sem,
    state_sem,
    gate_ss,
    gate_rs,
    pair_ss,
    pair_rs,
    cross_ss,
    cross_rs,
    ag_ss,
    relay_ss,
    ag_rs,
    half_ss,
    half_rs,
    y_ss,
    y_rs,
    full_ss,
    full_rs,
    sq_ss,
    sq_rs,
    up_ss,
    up_rs,
    upx_ss,
    upx_rs,
    hid_ss,
    hid_rs,
):
    me = lax.axis_index("kv")
    tme = lax.axis_index("tp")
    total, local = x_ref.shape
    rows, heads, dqk = norm_ref.shape
    dv = v_hbm.shape[1] // heads
    model = local * kvn
    hidden_units = up_hbm.shape[1]
    hp = gate_send.shape[0] // 3
    gate_width = gate_heads * dv
    gate_chunks = heads // gate_heads
    chunks = heads + gate_chunks
    up_chunks = hidden_units // up_width
    npairs = kvn // 2
    pair = me // 2
    partner = me + 1 - 2 * (me % 2)
    lead_bit = 1 - (2 * pair) // npairs
    leader = (me % 2) == lead_bit
    outer = (me % 2) != lead_bit

    def wrap(j):
        return lax.rem(me + j, kvn)

    def remote(src, dst, ssem, rsem, axis, peer):
        return pltpu.make_async_remote_copy(
            src_ref=src,
            dst_ref=dst,
            send_sem=ssem,
            recv_sem=rsem,
            device_id={axis: peer},
            device_id_type=MESH,
        )

    def arrived(dst, rsem, ssem):
        remote(dst, dst, ssem, rsem, "kv", partner).wait_recv()

    def outside():
        for jj in range(1, npairs):
            other = lax.rem(pair + jj, npairs)
            for b in range(2):
                yield jj, b, 2 * other + b

    small = []
    for i, (src, dst) in enumerate(
        (
            (x_hbm, x_ref),
            (gain_hbm, gain_ref),
            (ig_hbm, ig_ref),
            (fg_hbm, fg_ref),
            (bias_hbm, bias_ref),
            (max_hbm, max_ref),
            (norm_hbm, norm_ref),
            (head_gain_hbm, head_gain_ref),
            (mix_gain_hbm, mix_gain_ref),
        )
    ):
        small.append(pltpu.make_async_copy(src, dst, small_sem.at[i]))
    for copy in small[:4]:
        copy.start()

    def qkv_loads(h):
        found = []
        at = 0
        for ref, extent in ((q_hbm, dqk), (k_hbm, dqk), (v_hbm, dv)):
            src = ref.at[:, pl.ds(pl.multiple_of(h * extent, extent), extent)]
            found.append(pltpu.make_async_copy(src, weights.at[gate_chunks + h, :, pl.ds(at, extent)], w_sem.at[gate_chunks + h]))
            at += extent
        return found

    def gate_load(c):
        src = o_hbm.at[:, pl.ds(pl.multiple_of(c * gate_width, gate_width), gate_width)]
        return pltpu.make_async_copy(src, weights.at[c, :, pl.ds(0, gate_width)], w_sem.at[c])

    for c in range(min(1, gate_chunks)):
        gate_load(c).start()

    def state_load(h):
        return pltpu.make_async_copy(state_hbm.at[:, h], state.at[:, h], state_sem.at[h])

    tp_steps = []
    s = 1
    while s < tpn:
        tp_steps.append(s)
        s *= 2

    def tp_peer(s):
        return tme + s - 2 * s * ((tme // s) % 2)

    barrier = pltpu.get_barrier_semaphore()
    for j in range(1, kvn):
        pl.semaphore_signal(barrier, inc=1, device_id={"kv": wrap(j)}, device_id_type=MESH)
    for s in tp_steps:
        pl.semaphore_signal(barrier, inc=1, device_id={"tp": tp_peer(s)}, device_id_type=MESH)

    def row_of(ref):
        pieces = [ref[i : i + 1, :].astype(F32) for i in range(ref.shape[0])]
        return jnp.concatenate(pieces, axis=1)

    def lane_row(col):
        return jnp.broadcast_to(col, (total, LANES)).T

    for copy in small[:4]:
        copy.wait()
    for c in range(1, gate_chunks):
        gate_load(c).start()
    for h in range(heads):
        for copy in qkv_loads(h):
            copy.start()
    for copy in small[4:]:
        copy.start()
    xf = x_ref[...].astype(F32)
    squares = jnp.sum(xf * xf, axis=1, keepdims=True)
    scaled[...] = (xf * row_of(gain_ref)).astype(BF16)
    gate_send[...] = jnp.zeros(gate_send.shape, F32)
    contract = (((1,), (1,)), ((), ()))
    for i, ref in enumerate((ig_ref, fg_ref)):
        gate_send[i * hp : i * hp + heads, :] = lax.dot_general(
            ref[...], scaled[...], contract, preferred_element_type=F32
        )
    gate_send[2 * hp : 3 * hp, :] = lane_row(squares)[0:hp, :]
    pl.semaphore_wait(barrier, (kvn - 1) + len(tp_steps))
    gate_copies = [
        remote(gate_send, gate_recv.at[j - 1], gate_ss.at[j - 1], gate_rs.at[j - 1], "kv", wrap(j))
        for j in range(1, kvn)
    ]
    for copy in gate_copies:
        copy.start()

    def kind(c):
        return jnp.minimum(c // gate_chunks, 1)

    def block(buf, c, d, wide):
        if wide == width:
            return buf.at[c, d]
        return buf.at[c, d, :, pl.ds(0, wide)]

    def outer_sends(c, wide):
        found = []
        dests = [d for _, _, d in outside()] + [partner]
        for d in dests:
            found.append(
                remote(
                    block(part_send, c, d, wide),
                    block(pair_recv, c, d, wide),
                    pair_ss.at[kind(c)],
                    pair_rs.at[c, d],
                    "kv",
                    partner,
                )
            )
        return found

    def inner_send(c, wide):
        return remote(
            block(part_send, c, partner, wide),
            block(pair_recv, c, partner, wide),
            pair_ss.at[kind(c)],
            pair_rs.at[c, partner],
            "kv",
            partner,
        )

    def project(c, wide):
        tile = min(512, wide)

        def body(i, carry):
            cols = pl.ds(pl.multiple_of(i * tile, tile), tile)
            res = jnp.dot(scaled[...], weights[c, :, cols], preferred_element_type=F32)
            part_send[c, :, :, cols] = res.reshape(kvn, rows, tile).astype(BF16)
            return carry

        lax.fori_loop(0, wide // tile, body, 0)

        @pl.when(jnp.logical_and(outer, c < AHEAD))
        def _():
            for copy in outer_sends(c, wide):
                copy.start()

        @pl.when(leader)
        def _():
            inner_send(c, wide).start()

    def gate_project(c, carry):
        gate_load(c).wait()
        project(c, gate_width)
        return carry

    lax.fori_loop(0, gate_chunks, gate_project, 0)

    def qkv_project(h, carry):
        whole = weights.at[gate_chunks + h]
        pltpu.make_async_copy(up_hbm.at[:, pl.ds(0, width)], whole, w_sem.at[gate_chunks + h]).wait()
        state_load(h).start()
        project(gate_chunks + h, width)
        return carry

    lax.fori_loop(0, heads, qkv_project, 0)

    wide_out = min(width, local)
    second = []
    for a in range(0, out_hbm.shape[0], local):
        for b in range(0, local, wide_out):
            second.append((out_hbm, a, b, wide_out))
    out_blocks = len(second)
    for b in range(0, hidden_units, width):
        second.append((up_hbm, 0, b, width))
    loads2 = []
    for i, (ref, a, b, wide) in enumerate(second):
        copy = pltpu.make_async_copy(
            ref.at[pl.ds(a, local), pl.ds(b, wide)], weights.at[i, :, pl.ds(0, wide)], w2_sem.at[i]
        )
        copy.start()
        loads2.append(copy)
    down_load = pltpu.make_async_copy(down_hbm, down_w, down_sem.at[0])
    down_load.start()

    for copy in small[4:]:
        copy.wait()
    for h in range(heads):
        norm_h[h] = norm_ref[:, h, :]
        n = dv // LANES
        for i in range(n):
            hg_rows[h, :, i * LANES : (i + 1) * LANES] = head_gain_ref[h * n + i : h * n + i + 1, :].astype(F32)
    max_pad[...] = jnp.zeros(max_pad.shape, F32)
    max_pad[0:heads, 0:rows] = max_ref[...]
    spread = jnp.broadcast_to(bias_ref[...], (heads, heads))
    diag = lax.broadcasted_iota(jnp.int32, (heads, heads), 0) == lax.broadcasted_iota(jnp.int32, (heads, heads), 1)
    bias = jnp.sum(jnp.where(diag, spread, 0.0), axis=1, keepdims=True)
    if heads < hp:
        bias = jnp.concatenate([bias, jnp.zeros((hp - heads, 1), F32)], axis=0)
    for copy in gate_copies:
        copy.wait_recv()
    gsum = gate_send[...]
    for j in range(1, kvn):
        gsum = gsum + gate_recv[j - 1]
    gsum = pltpu.roll(gsum, lax.rem(total - me * rows, total), 1)
    scale = lax.rsqrt(gsum[2 * hp : 3 * hp, :] / model + EPS)
    igate = gsum[0:hp, :] * scale
    z = gsum[hp : 2 * hp, :] * scale + bias
    logf = jnp.minimum(z, 0.0) - jnp.log1p(jnp.exp(-jnp.abs(z)))
    held = logf + max_pad[...]
    new_max = jnp.maximum(held, igate)
    new_max_ref[...] = new_max[0:heads, 0:rows]
    fdec = jnp.exp(held - new_max)
    idec = jnp.exp(igate - new_max)
    floor = jnp.exp(-new_max)
    stacked = jnp.concatenate([fdec, idec, floor, scale, jnp.zeros((LANES - 4 * hp, total), F32)], axis=0).T
    for h in range(heads):
        for i, dst in enumerate((fd_all, id_all, em_all)):
            at = i * hp + h
            dst[h] = jnp.broadcast_to(stacked[0:rows, at : at + 1], (rows, LANES))
    scale_b[...] = jnp.broadcast_to(stacked[0:rows, 3 * hp : 3 * hp + 1], (rows, LANES))

    def cross_sends(c, wide):
        found = []
        for jj, b, d in outside():
            slot = npairs - jj - 1
            found.append(
                (
                    d,
                    remote(
                        block(pair_recv, c, d, wide),
                        block(cross_recv, c, slot, wide),
                        cross_ss.at[kind(c)],
                        cross_rs.at[c, slot],
                        "kv",
                        d,
                    ),
                )
            )
        return found

    def combine(c, wide):
        for d, copy in cross_sends(c, wide):
            arrived(block(pair_recv, c, d, wide), pair_rs.at[c, d], pair_ss.at[0])
            cols = pl.ds(0, wide)
            both = part_send[c, d, :, cols].astype(F32) + pair_recv[c, d, :, cols].astype(F32)
            pair_recv[c, d, :, cols] = both.astype(BF16)
            copy.start()

    def combine_any(c):
        @pl.when(leader)
        def _():
            if gate_width == width:

                @pl.when(c < chunks)
                def _():
                    combine(c, width)

            else:

                @pl.when(c < gate_chunks)
                def _():
                    combine(c, gate_width)

                @pl.when(jnp.logical_and(c >= gate_chunks, c < chunks))
                def _():
                    combine(c, width)

    def send_ahead(c):
        @pl.when(outer)
        def _():
            if gate_width == width:

                @pl.when(c < chunks)
                def _():
                    for copy in outer_sends(c, width):
                        copy.start()

            else:

                @pl.when(c < gate_chunks)
                def _():
                    for copy in outer_sends(c, gate_width):
                        copy.start()

                @pl.when(jnp.logical_and(c >= gate_chunks, c < chunks))
                def _():
                    for copy in outer_sends(c, width):
                        copy.start()

    def summed(c, wide):
        arrived(block(pair_recv, c, me, wide), pair_rs.at[c, me], pair_ss.at[0])
        for i in range(npairs - 1):
            arrived(block(cross_recv, c, i, wide), cross_rs.at[c, i], pair_ss.at[0])
        found = []
        for g in range(0, wide, LANES):
            cols = pl.ds(g, LANES)
            val = part_send[c, me, :, cols].astype(F32) + pair_recv[c, me, :, cols].astype(F32)
            for i in range(npairs - 1):
                val = val + cross_recv[c, i, :, cols].astype(F32)
            found.append((val * scale_b[...]).astype(BF16).astype(F32))
        return found

    last = heads - 1

    def final(h):
        return (h + 1) // heads

    def own_sends(h):
        src = merged_all.at[h, me]
        return [
            remote(src, src, ag_ss.at[final(h)], ag_rs.at[h, me], "kv", wrap(j)) for j in range(1, kvn)
        ]

    def outer_own(h):
        src = merged_all.at[h, me]
        return remote(src, src, ag_ss.at[final(h)], ag_rs.at[h, me], "kv", partner)

    def relay_sends(h):
        src = merged_all.at[h, partner]
        return [
            remote(src, src, relay_ss.at[0], ag_rs.at[h, partner], "kv", d)
            for jj, b, d in outside()
        ]

    def relay(h):
        @pl.when(leader)
        def _():
            arrived(merged_all.at[h, partner], ag_rs.at[h, partner], ag_ss.at[0])
            for copy in relay_sends(h):
                copy.start()

    def spread_merged(h):
        direct = jnp.logical_or(leader, h == last)

        @pl.when(direct)
        def _():
            for copy in own_sends(h):
                copy.start()

        @pl.when(jnp.logical_not(direct))
        def _():
            outer_own(h).start()

    out_tile = min(256, wide_out)
    out_cols = local // wide_out

    def out_project(batch, first):
        for h in batch:
            for _, _, d in outside():
                arrived(merged_all.at[h, d], ag_rs.at[h, d], ag_ss.at[0])

            @pl.when(jnp.logical_or(outer, h == last))
            def _(h=h):
                arrived(merged_all.at[h, partner], ag_rs.at[h, partner], ag_ss.at[0])

        for b in range(out_cols):

            def body(t, carry, b=b):
                cols = pl.ds(pl.multiple_of(t * out_tile, out_tile), out_tile)
                into = pl.ds(pl.multiple_of(b * wide_out + t * out_tile, out_tile), out_tile)
                acc = jnp.zeros((total, out_tile), F32)
                for h in batch:
                    slot = (h * dv // local) * out_cols + b
                    at = (h * dv) % local
                    lhs = merged_all[h].reshape(total, dv)
                    acc = acc + jnp.dot(lhs, weights[slot, at : at + dv, cols], preferred_element_type=F32)
                if first:
                    part[:, into] = acc
                else:
                    part[:, into] += acc
                return carry

            lax.fori_loop(0, wide_out // out_tile, body, 0)

    for c in range(SKEW):
        combine_any(c)

    def gate_body(c, carry):
        combine_any(c + SKEW)
        cols = summed(c, gate_width)
        n = dv // LANES
        for i in range(gate_heads):
            o = jnp.concatenate(cols[i * n : (i + 1) * n], axis=1)
            opened[c * gate_heads + i] = jax.nn.sigmoid(o)
        send_ahead(c + AHEAD)
        return carry

    lax.fori_loop(0, gate_chunks, gate_body, 0)
    def head_body(h, carry):
        combine_any(gate_chunks + h + SKEW)
        cols = summed(gate_chunks + h, width)
        nq = dqk // LANES
        q = jnp.concatenate(cols[:nq], axis=1) * (dqk ** (-0.5))
        k = jnp.concatenate(cols[nq : 2 * nq], axis=1)
        v = jnp.concatenate(cols[2 * nq :], axis=1)
        fd = fd_all[h]
        ik = id_all[h] * k
        nn = fd * norm_h[h] + ik
        norm_h[h] = nn
        denom = jnp.sum(q * nn, axis=1, keepdims=True)
        pad = jnp.zeros((LANES - 2 * rows, dqk), F32)
        turned = jnp.concatenate([ik, q, pad], axis=0).T
        wide_fd = jnp.concatenate([fd] * (dv // LANES), axis=1)
        state_load(h).wait()
        for r in range(rows):
            new = wide_fd[r : r + 1, :] * state[r, h] + turned[:, r : r + 1] * v[r : r + 1, :]
            state[r, h] = new
            numer_s[r : r + 1, :] = jnp.sum(turned[:, rows + r : rows + r + 1] * new, axis=0, keepdims=True)
        readout = numer_s[...] / jnp.maximum(jnp.abs(denom), em_all[h][:, 0:1])
        normed = readout * lax.rsqrt(jnp.sum(readout * readout, axis=1, keepdims=True) / dv + EPS)
        merged_all[h, me] = (opened[h] * (normed * hg_rows[h])).astype(BF16)
        spread_merged(h)

        send_ahead(gate_chunks + h + AHEAD)
        for early in range(last):
            when = min(early + 3, (early + heads + 1) // 2, last)

            @pl.when(h == when)
            def _(early=early):
                relay(early)

        return carry

    lax.fori_loop(0, heads, head_body, 0)
    for copy in loads2[:out_blocks]:
        copy.wait()
    late = max(heads - 2, 0)
    if late:
        out_project(range(late), True)
    out_project(range(late, heads), late == 0)

    half = total // 2
    piece = local // PIECES
    low = tme % 2
    mate = tme + 1 - 2 * low
    mine = pl.ds(pl.multiple_of(low * half, half), half)
    theirs = pl.ds(pl.multiple_of((1 - low) * half, half), half)

    def tp_sum(n, base):
        sent = []
        stage = []
        for p in range(PIECES):
            cols = slice(p * piece, (p + 1) * piece)
            half_send[n, p] = part[theirs, cols].astype(BF16)
            copy = remote(half_send.at[n, p], half_recv.at[n, p], half_ss.at[n, p], half_rs.at[n, p], "tp", mate)
            copy.start()
            stage.append(copy)
        sent += stage
        for p in range(PIECES):
            cols = slice(p * piece, (p + 1) * piece)
            stage[p].wait_recv()
            val = part[mine, cols] + half_recv[n, p].astype(F32)
            if len(tp_steps) > 1:
                y_send[n, 0, p] = val.astype(BF16)
            else:
                full[n, low, p] = (base(p) + val).astype(BF16)
        for i, s in enumerate(tp_steps[1:]):
            stage = []
            for p in range(PIECES):
                copy = remote(
                    y_send.at[n, i, p], y_recv.at[n, i, p], y_ss.at[n, i, p], y_rs.at[n, i, p], "tp", tp_peer(s)
                )
                copy.start()
                stage.append(copy)
            sent += stage
            for p in range(PIECES):
                stage[p].wait_recv()
                val = y_send[n, i, p].astype(F32) + y_recv[n, i, p].astype(F32)
                if i + 2 < len(tp_steps):
                    y_send[n, i + 1, p] = val.astype(BF16)
                else:
                    full[n, low, p] = (base(p) + val).astype(BF16)
        stage = []
        for p in range(PIECES):
            src = full.at[n, low, p]
            copy = remote(src, src, full_ss.at[n, p], full_rs.at[n, p], "tp", mate)
            copy.start()
            stage.append(copy)
        for copy in stage:
            copy.wait_recv()
        return sent + stage

    sent = tp_sum(0, lambda p: x_ref[mine, p * piece : (p + 1) * piece].astype(F32))
    mix_row = row_of(mix_gain_ref)
    sq = jnp.zeros((total, 1), F32)
    for p in range(PIECES):
        cols = slice(p * piece, (p + 1) * piece)
        rf = jnp.concatenate([full[0, 0, p], full[0, 1, p]], axis=0).astype(F32)
        sq = sq + jnp.sum(rf * rf, axis=1, keepdims=True)
        scaled[:, cols] = (rf * mix_row[:, cols]).astype(BF16)
    sq_send[...] = lane_row(sq)[0:8, :]
    sq_copies = [
        remote(sq_send, sq_recv.at[j - 1], sq_ss.at[j - 1], sq_rs.at[j - 1], "kv", wrap(j)) for j in range(1, kvn)
    ]
    for copy in sq_copies:
        copy.start()

    for copy in loads2[out_blocks:]:
        copy.wait()
    per_slot = width // up_width

    def outer_up(c):
        return remote(upb.at[0, c], upb.at[1, c], up_ss.at[0], up_rs.at[c], "kv", partner)

    def up_body(c, carry):
        slot = out_blocks + c // per_slot
        cols = pl.ds(pl.multiple_of((c % per_slot) * up_width, up_width), up_width)
        upb[0, c] = jnp.dot(scaled[...], weights[slot, :, cols], preferred_element_type=F32).astype(BF16)

        @pl.when(outer)
        def _():
            outer_up(c).start()

        return carry

    lax.fori_loop(0, up_chunks, up_body, 0)
    for copy in sq_copies:
        copy.wait_recv()
    sq_sum = sq_send[...]
    for j in range(1, kvn):
        sq_sum = sq_sum + sq_recv[j - 1]
    two = lax.rsqrt(sq_sum[0:1, :] / model + EPS)
    scale_two[...] = jnp.broadcast_to(two, (LANES, total)).T

    def up_cross_sends(c):
        found = []
        for jj in range(1, npairs):
            other = lax.rem(pair + jj, npairs)
            head = 2 * other + 1 - (2 * other) // npairs
            slot = npairs - jj - 1
            found.append(
                remote(upb.at[1, c], up_cross.at[c, slot], upx_ss.at[0], upx_rs.at[c, slot], "kv", head)
            )
        return found

    def hidden_send(c):
        return remote(upb.at[0, c], upb.at[1, c], hid_ss.at[0], hid_rs.at[c], "kv", partner)

    def up_combine(c):
        arrived(upb.at[1, c], up_rs.at[c], up_ss.at[0])
        both = upb[0, c].astype(F32) + upb[1, c].astype(F32)
        upb[1, c] = both.astype(BF16)
        for copy in up_cross_sends(c):
            copy.start()

    def up_finish(c):
        for i in range(npairs - 1):
            arrived(up_cross.at[c, i], upx_rs.at[c, i], up_ss.at[0])
        for g in range(0, up_width, LANES):
            cols = pl.ds(g, LANES)
            val = upb[1, c, :, cols].astype(F32)
            for i in range(npairs - 1):
                val = val + up_cross[c, i, :, cols].astype(F32)
            act = jnp.maximum(val * scale_two[...], 0.0)
            upb[0, c, :, cols] = (act * act).astype(BF16)
        hidden_send(c).start()

    down_load.wait()
    down_tile = min(256, local)
    part[...] = jnp.zeros(part.shape, F32)

    def down_project(c, which):
        rws = pl.ds(pl.multiple_of(c * up_width, up_width), up_width)

        def body(t, carry):
            cols = pl.ds(pl.multiple_of(t * down_tile, down_tile), down_tile)
            part[:, cols] += jnp.dot(upb[which, c], down_w[rws, cols], preferred_element_type=F32)
            return carry

        lax.fori_loop(0, local // down_tile, body, 0)

    @pl.when(leader)
    def _():
        def tick(c, carry):
            @pl.when(c < up_chunks)
            def _():
                up_combine(c)

            @pl.when(c >= UP_SKEW)
            def _():
                up_finish(c - UP_SKEW)
                down_project(c - UP_SKEW, 0)

            return carry

        lax.fori_loop(0, up_chunks + UP_SKEW, tick, 0)

    @pl.when(outer)
    def _():
        def tick(c, carry):
            arrived(upb.at[1, c], hid_rs.at[c], up_ss.at[0])
            down_project(c, 1)
            return carry

        lax.fori_loop(0, up_chunks, tick, 0)

    def resid(p):
        return full[0, low, p].astype(F32)

    sent += tp_sum(1, resid)
    for p in range(PIECES):
        cols = slice(p * piece, (p + 1) * piece)
        for b in range(2):
            mixed_ref[b * half : (b + 1) * half, cols] = full[1, b, p]
    for h in range(heads):
        new_norm_ref[:, h, :] = norm_h[h]

    for copy in sent + gate_copies + sq_copies:
        copy.wait_send()

    def sent_all(ref, ssem):
        remote(ref, ref, ssem, pair_rs.at[0, 0], "kv", partner).wait_send()

    def projections(n):
        gate_part = part_send.at[pl.ds(0, gate_chunks), pl.ds(0, n), :, pl.ds(0, gate_width)]
        return gate_part, part_send.at[pl.ds(gate_chunks, heads), pl.ds(0, n)]

    def readouts(first, count, n):
        return merged_all.at[pl.ds(first, count), pl.ds(0, n)]

    others = kvn - 1
    beyond = kvn - 2

    @pl.when(outer)
    def _():
        for i, ref in enumerate(projections(others)):
            sent_all(ref, pair_ss.at[i])
        if last:
            sent_all(readouts(0, last, 1), ag_ss.at[0])
        sent_all(readouts(last, 1, others), ag_ss.at[1])
        sent_all(upb.at[0], up_ss.at[0])

    @pl.when(leader)
    def _():
        for i, ref in enumerate(projections(1)):
            sent_all(ref, pair_ss.at[i])
        if last:
            sent_all(readouts(0, last, others), ag_ss.at[0])
        sent_all(readouts(last, 1, others), ag_ss.at[1])
        if beyond:
            for i, ref in enumerate(projections(beyond)):
                sent_all(ref, cross_ss.at[i])
            if last:
                sent_all(readouts(0, last, beyond), relay_ss.at[0])
            sent_all(up_cross, upx_ss.at[0])
        sent_all(upb.at[0], hid_ss.at[0])


def flush(*refs):
    sem = refs[-1]
    n = (len(refs) - 1) // 2
    copies = []
    for i in range(1, n):
        copies.append((refs[i], refs[n + i]))
    for r in range(refs[0].shape[0]):
        copies.append((refs[0].at[r], refs[n].at[r]))
    started = []
    for i, (src, dst) in enumerate(copies):
        copy = pltpu.make_async_copy(src, dst, sem.at[i])
        copy.start()
        started.append(copy)
    for copy in started:
        copy.wait()


def per_device(
    kvn,
    tpn,
    x_rows,
    in_gain,
    query_weight,
    key_weight,
    value_weight,
    outgate_weight,
    input_gate_weight,
    forget_gate_weight,
    forget_bias,
    state_matrix,
    state_norm,
    state_max,
    head_gain,
    out_weight,
    mix_gain,
    up_weight,
    down_weight,
):
    total, local = x_rows.shape
    rows, heads, dqk, dv = state_matrix.shape
    hidden_units = up_weight.shape[1]
    width = 2 * dqk + dv
    gate_heads = min(2, heads)
    gate_width = gate_heads * dv
    gate_chunks = heads // gate_heads
    chunks = heads + gate_chunks
    up_width = min(256, width)
    up_chunks = hidden_units // up_width
    wide_out = min(width, local)
    slots2 = (heads * dv // local) * (local // wide_out) + hidden_units // width
    slots = max(chunks, slots2)
    hp = -(-heads // 8) * 8
    npairs = kvn // 2
    np1 = max(npairs - 1, 1)
    steps = max((tpn - 1).bit_length() - 1, 1)
    half, piece = total // 2, local // PIECES
    vmem = pl.BlockSpec(memory_space=pltpu.VMEM)
    hbm = pl.BlockSpec(memory_space=pl.ANY)
    V = pltpu.VMEM
    dma = pltpu.SemaphoreType.DMA
    k1 = kvn - 1
    gains = (local // LANES, LANES)
    hg_shape = (heads * dv // LANES, LANES)
    scratch = [
        V((total, local), BF16),
        V(gains, BF16),
        V((heads, local), BF16),
        V((heads, local), BF16),
        V((1, heads), F32),
        V((rows, heads, dqk), F32),
        V((heads, rows), F32),
        V(hg_shape, BF16),
        V(gains, BF16),
        V((slots, local, width), BF16),
        V((hidden_units, local), BF16),
        V((total, local), BF16),
        V((total, local), F32),
        V((3 * hp, total), F32),
        V((k1, 3 * hp, total), F32),
        V((hp, total), F32),
        V((chunks, kvn, rows, width), BF16),
        V((chunks, kvn, rows, width), BF16),
        V((chunks, np1, rows, width), BF16),
        V((heads, rows, dqk), F32),
        V((heads, rows, LANES), F32),
        V((heads, rows, LANES), F32),
        V((heads, rows, LANES), F32),
        V((rows, LANES), F32),
        V((heads, 1, dv), F32),
        V((rows, dv), F32),
        V((heads, rows, dv), F32),
        V((heads, kvn, rows, dv), BF16),
        V((2, PIECES, half, piece), BF16),
        V((2, PIECES, half, piece), BF16),
        V((2, steps, PIECES, half, piece), BF16),
        V((2, steps, PIECES, half, piece), BF16),
        V((2, 2, PIECES, half, piece), BF16),
        V((8, total), F32),
        V((k1, 8, total), F32),
        V((total, LANES), F32),
        V((2, up_chunks, total, up_width), BF16),
        V((up_chunks, np1, total, up_width), BF16),
        dma((9,)),
        dma((chunks,)),
        dma((slots2,)),
        dma((1,)),
        dma((heads,)),
        dma((k1,)),
        dma((k1,)),
        dma((2,)),
        dma((chunks, kvn)),
        dma((2,)),
        dma((chunks, np1)),
        dma((2,)),
        dma((1,)),
        dma((heads, kvn)),
        dma((2, PIECES)),
        dma((2, PIECES)),
        dma((2, steps, PIECES)),
        dma((2, steps, PIECES)),
        dma((2, PIECES)),
        dma((2, PIECES)),
        dma((k1,)),
        dma((k1,)),
        dma((1,)),
        dma((up_chunks,)),
        dma((1,)),
        dma((up_chunks, np1)),
        dma((1,)),
        dma((up_chunks,)),
    ]
    state_bytes = state_matrix.size * 4
    outs = pl.pallas_call(
        functools.partial(kernel, kvn, tpn, width, gate_heads, up_width),
        out_shape=(
            pltpu.VMEM((total, local), BF16),
            pltpu.VMEM(state_matrix.shape, F32),
            pltpu.VMEM(state_norm.shape, F32),
            pltpu.VMEM((heads, rows), F32),
        ),
        in_specs=[hbm] * 17,
        out_specs=(vmem,) * 4,
        scratch_shapes=scratch,
        compiler_params=pltpu.CompilerParams(
            collective_id=0,
            has_side_effects=True,
            vmem_limit_bytes=67043328 - state_bytes - (1 << 19),
        ),
    )(
        x_rows,
        in_gain.reshape(gains),
        query_weight,
        key_weight,
        value_weight,
        outgate_weight,
        input_gate_weight.T,
        forget_gate_weight.T,
        forget_bias.reshape(1, heads),
        state_matrix,
        state_norm,
        state_max.T,
        head_gain.reshape(hg_shape),
        out_weight,
        mix_gain.reshape(gains),
        up_weight,
        down_weight,
    )
    mixed, new_matrix, new_norm, new_max = outs
    new_matrix, mixed = pl.pallas_call(
        flush,
        out_shape=(jax.ShapeDtypeStruct(state_matrix.shape, F32), jax.ShapeDtypeStruct((total, local), BF16)),
        in_specs=[hbm] * 2,
        out_specs=(hbm,) * 2,
        scratch_shapes=[dma((rows + 3,))],
        compiler_params=pltpu.CompilerParams(vmem_limit_bytes=1 << 20),
    )(new_matrix, mixed)
    return (mixed, new_matrix, new_norm, new_max.T)


def solution(mesh):
    placed = (
        P("grp", "kv"),
        P("kv"),
        P("kv", "tp"),
        P("kv", "tp"),
        P("kv", "tp"),
        P("kv", "tp"),
        P("kv", "tp"),
        P("kv", "tp"),
        P("tp"),
        P(("grp", "kv"), "tp", None, None),
        P(("grp", "kv"), "tp", None),
        P(("grp", "kv"), "tp"),
        P("tp"),
        P("tp", "kv"),
        P("kv"),
        P("kv", "tp"),
        P("tp", "kv"),
    )
    return jax.shard_map(
        functools.partial(per_device, mesh.shape["kv"], mesh.shape["tp"]),
        mesh=mesh,
        in_specs=placed,
        out_specs=(
            P("grp", "kv"),
            P(("grp", "kv"), "tp", None, None),
            P(("grp", "kv"), "tp", None),
            P(("grp", "kv"), "tp"),
        ),
        check_vma=False,
    )
```
